32 devices in a mesh: ep: 8 (over z, core), tp: 4 (over y, x).
Axes of the slice: x: 2, y: 2, z: 4, core: 2. Of those that a mesh axis runs over, the one named last changes fastest.
Arguments:
- tokens: bfloat16 [1024, 2048], P('ep', 'tp'), may hold values from -3000 to 3000
- norm_gain: float32 [2048], replicated, may hold values from 0.1 to 1.9
- gate_weight: bfloat16 [8, 2048, 512], P('ep'), may hold values from -0.125 to 0.125
- up_weight: bfloat16 [8, 2048, 512], P('ep'), may hold values from -0.125 to 0.125
- down_weight: bfloat16 [8, 512, 2048], P('ep'), may hold values from -0.25 to 0.25
- expert_ids: int32 [1024, 2], P('ep'), may hold values from 0 to 7, as said below
- route_weight: float32 [1024, 2], P('ep'), may hold values from 0.2 to 1
Outputs:
- mixed: bfloat16 [1024, 2048], P('ep', 'tp')
The draws below stay inside these ranges and needn't reach their ends.
Inputs may be any that keep to these rules, and one draw needn't show every extreme that they name: `expert_ids`: A token's two experts differ and lie in one group of 2 consecutive experts. In each aligned block of 32 rows no expert is named more than 16 times, and in every block all experts of one group, the same group for all blocks, are named exactly 16 times.
All inputs are finite; a program needn't handle non-finite values.
Results may differ from the reference program's by a relative error of at most 0.0071.
Values may be sent and summed in bfloat16 or wider, within the bound.
A program may use at most 64 MiB of HBM per device.

```python
import math
import jax
import jax.numpy as jnp
from jax import lax

D = 2048
FF = 512
TOK_DEV = 32
EXPERTS = 8
EPG = 2
GROUPS = 4
CAP = 16
GCAP = 16
TOKENS = 1024


def group_order(order_key):
    return jax.random.permutation(order_key, EPG)


def route_block(block_key, hot_group):
    keys = jax.random.split(block_key, 5)
    group_bias = jax.random.randint(keys[0], (GROUPS,), 1, 5)
    slot_group = jnp.arange(GROUPS * GCAP, dtype=jnp.int32) // GCAP
    score = jax.random.randint(keys[1], (GROUPS * GCAP,), 0, 65536) * group_bias[slot_group]
    score = jnp.where(slot_group == hot_group, 4194304, score)
    score = score * (GROUPS * GCAP) + jnp.arange(GROUPS * GCAP, dtype=jnp.int32)
    unused, chosen = lax.top_k(score, TOK_DEV)
    chosen = chosen[jax.random.permutation(keys[2], TOK_DEV)]
    group_of = chosen // GCAP
    within = chosen % GCAP
    orders = jax.vmap(group_order)(jax.random.split(keys[3], GROUPS))
    offsets = jax.random.randint(keys[4], (GROUPS, CAP // 2), 1, EPG)
    position = within % EPG
    first = orders[group_of, position]
    second = orders[group_of, (position + offsets[group_of, within // EPG]) % EPG]
    return jnp.stack([group_of * EPG + first, group_of * EPG + second], axis=1).astype(jnp.int32)


def draw_expert_ids(key, part):
    hot_group = jax.random.randint(jax.random.fold_in(key, 11), (), 0, GROUPS)
    block_keys = jax.random.split(jax.random.fold_in(key, 12), TOKENS // TOK_DEV)
    blocks = jax.vmap(route_block, in_axes=(0, None))(block_keys, hot_group)
    return blocks.reshape(TOKENS, 2)


def draw_tokens(key, part):
    keys = jax.random.split(jax.random.fold_in(key, 21), 4)
    column_rise = jnp.exp(jnp.log(10.0) * jnp.arange(D, dtype=jnp.float32) / D)
    column_rough = jnp.exp(jax.random.uniform(keys[0], (D,), jnp.float32, -0.5, 0.5))
    row_scale = jnp.exp(jax.random.uniform(keys[1], (TOKENS, 1), jnp.float32, 0.0, jnp.log(10.0)))
    base = jnp.clip(jax.random.normal(keys[3], (TOKENS, D), jnp.float32), -6.0, 6.0)
    return (base * row_scale * column_rise * column_rough).astype(jnp.bfloat16)


def shard_levels(stream_key, extent, shards, low, largest):
    loudness = 1.0
    for dim, parts in shards:
        steps = jax.random.uniform(jax.random.fold_in(jax.random.fold_in(stream_key, 6), dim), (parts,), jnp.float32, low / len(shards), largest / len(shards))
        loudness = loudness * jnp.repeat(jnp.exp(steps), extent[dim] // parts).reshape((-1,) + (1,) * (len(extent) - 1 - dim))
    return loudness


def centred(stream_key, extent, deviation, reach, cuts=(), held_as=jnp.bfloat16):
    array = jax.random.normal(stream_key, extent, jnp.float32) * deviation
    if len(cuts) > 0:
        array = shard_levels(stream_key, extent, cuts, -0.22, 0.18) * array
    return jnp.clip(array, min=-reach, max=reach).astype(held_as)


def setup_inputs(seed: int = 0) -> dict:
    key_of = jax.random.split(jax.random.key(seed), 8)
    tokens = draw_tokens(jax.random.fold_in(key_of[7], 71), 0)
    norm_gain = jnp.clip(1.0 + 0.18 * jax.random.normal(key_of[1], (D,), jnp.float32), 0.1, 1.9)
    gate_weight = centred(key_of[2], (EXPERTS, D, FF), D ** -0.5, 0.125, ((0, 8),))
    up_weight = centred(key_of[3], (EXPERTS, D, FF), D ** -0.5, 0.125, ((0, 8),))
    down_weight = centred(key_of[4], (EXPERTS, FF, D), FF ** -0.5, 0.25, ((0, 8),))
    expert_ids = draw_expert_ids(jax.random.fold_in(key_of[7], 71), 0)
    route_weight = jnp.clip(jnp.exp(math.log(1.0) - 1.609438 * jax.random.uniform(key_of[6], (TOKENS, 2), jnp.float32) ** shard_levels(key_of[6], (TOKENS, 2), ((0, 8),), -0.2, 0.2)), 0.2, 1.0)
    return {"tokens": tokens, "norm_gain": norm_gain, "gate_weight": gate_weight, "up_weight": up_weight, "down_weight": down_weight, "expert_ids": expert_ids, "route_weight": route_weight}


def reference(tokens, norm_gain, gate_weight, up_weight, down_weight, expert_ids, route_weight):
    widened = tokens.astype(jnp.float32)
    mean_square = lax.optimization_barrier(jnp.mean(widened * widened, axis=-1, keepdims=True))
    normed = (widened * lax.rsqrt(mean_square + 1e-06) * norm_gain).astype(jnp.bfloat16)
    flat_ids = expert_ids.reshape(-1)
    flat_weight = route_weight.reshape(-1)
    longest = TOKENS // TOK_DEV * CAP

    def per_expert(summed, expert):
        matches = flat_ids == expert
        places = jnp.nonzero(matches, size=longest, fill_value=0)[0].astype(jnp.int32)
        present = jnp.arange(longest, dtype=jnp.int32) < jnp.sum(matches.astype(jnp.int32))
        token_rows = places // 2
        chosen = normed[token_rows]
        gate_part = jnp.dot(chosen, gate_weight[expert], preferred_element_type=jnp.float32)
        up_part = jnp.dot(chosen, up_weight[expert], preferred_element_type=jnp.float32)
        hidden = (jax.nn.silu(gate_part) * up_part).astype(jnp.bfloat16)
        produced = jnp.dot(hidden, down_weight[expert], preferred_element_type=jnp.float32).astype(jnp.bfloat16)
        produced = lax.optimization_barrier(produced).astype(jnp.float32)
        weight_used = jnp.where(present, flat_weight[places], 0.0)
        summed = summed.at[token_rows].add(produced * weight_used[:, None])
        return (summed, None)
    summed, unused = lax.scan(per_expert, jnp.zeros((TOKENS, D), jnp.float32), jnp.arange(EXPERTS, dtype=jnp.int32))
    return summed.astype(jnp.bfloat16)
```

```python
import math
from functools import partial

import jax
import jax.numpy as jnp
from jax import lax
from jax.experimental import pallas as pl
from jax.experimental.pallas import tpu as pltpu
from jax.sharding import PartitionSpec as P


def slot_numbers(block_ids, experts):
    flat_ids = block_ids.reshape(-1)
    hit_table = (flat_ids[:, None] == jnp.arange(experts, dtype=jnp.int32)[None, :]).astype(
        jnp.int32
    )
    earlier = jnp.cumsum(hit_table, axis=0) - hit_table
    return (flat_ids, jnp.sum(earlier * hit_table, axis=1))


def placement_matrix(flat_ids, slot_index, experts, capacity):
    target = (flat_ids * capacity + slot_index).reshape(-1, 2)
    slot_rows = jnp.arange(experts * capacity, dtype=jnp.int32)[:, None]
    first_hit = (target[:, 0][None, :] == slot_rows).astype(jnp.bfloat16)
    second_hit = (target[:, 1][None, :] == slot_rows).astype(jnp.bfloat16)
    return first_hit + second_hit


def expert_apply(row_data, gate_weight, up_weight, down_weight):
    shape_in = row_data.shape
    flat_rows = row_data.reshape(-1, shape_in[-1])
    gate_part = jnp.dot(flat_rows, gate_weight[0], preferred_element_type=jnp.float32)
    up_part = jnp.dot(flat_rows, up_weight[0], preferred_element_type=jnp.float32)
    hidden = (jax.nn.silu(gate_part) * up_part).astype(jnp.bfloat16)
    produced = jnp.dot(hidden, down_weight[0], preferred_element_type=jnp.float32).astype(
        jnp.bfloat16
    )
    return produced.reshape(shape_in[:-1] + (produced.shape[-1],))


def local(tokens, norm_gain, gate_weight, up_weight, down_weight, expert_ids, route_weight):
    tp_count = lax.axis_size("tp")
    experts = lax.axis_size("ep") * gate_weight.shape[0]
    model_width = gate_weight.shape[1]
    group_rows = tokens.shape[0]
    block_rows = group_rows // tp_count
    capacity = 4 * block_rows // experts
    tp_index = lax.axis_index("tp")
    apply_experts = partial(
        expert_apply, gate_weight=gate_weight, up_weight=up_weight, down_weight=down_weight
    )
    full_rows = lax.all_to_all(tokens, "tp", split_axis=0, concat_axis=1, tiled=True)
    block_ids = lax.dynamic_slice_in_dim(expert_ids, tp_index * block_rows, block_rows, 0)
    block_weight = lax.dynamic_slice_in_dim(route_weight, tp_index * block_rows, block_rows, 0)
    widened = full_rows.astype(jnp.float32)
    mean_square = jnp.mean(widened * widened, axis=-1, keepdims=True)
    normed = (widened * lax.rsqrt(mean_square + 1e-06) * norm_gain).astype(jnp.bfloat16)
    flat_ids, slot_index = slot_numbers(block_ids, experts)
    placing = placement_matrix(flat_ids, slot_index, experts, capacity)
    outgoing = jnp.dot(placing, normed, preferred_element_type=jnp.float32).astype(jnp.bfloat16)
    outgoing = outgoing.reshape(experts, capacity, model_width)
    produced = apply_experts(
        lax.all_to_all(outgoing, "ep", split_axis=0, concat_axis=0, tiled=True)
    )
    returned = lax.all_to_all(produced, "ep", split_axis=0, concat_axis=0, tiled=True)
    picked = jnp.take(returned.reshape(-1, model_width), flat_ids * capacity + slot_index, axis=0)
    weighted = picked.astype(jnp.float32) * block_weight.reshape(-1)[:, None]
    mixed_rows = weighted.reshape(block_rows, 2, model_width).sum(axis=1).astype(jnp.bfloat16)
    return lax.all_to_all(mixed_rows, "tp", split_axis=1, concat_axis=0, tiled=True)


def direct_kernel(
    dims,
    ids_hbm,
    mix_hbm,
    tok_hbm,
    gain_hbm,
    gate_hbm,
    up_hbm,
    down_hbm,
    out_ref,
    ids_ref,
    mix_ref,
    tok_ref,
    gain_ref,
    pick_buf,
    send_buf,
    weight_send,
    row_buf,
    wide_buf,
    down_buf,
    hidden_buf,
    result_buf,
    back_buf,
    load_sem,
    row_send_sem,
    row_recv_sem,
    weight_send_sem,
    pass_send_sem,
    pass_recv_sem,
    pair_send_sem,
    pair_recv_sem,
    down_send_sem,
    down_recv_sem,
    back_send_sem,
    back_recv_sem,
):
    ep_count, tp_count, group, cap = dims
    chips = ep_count // group
    rows, width = tok_ref.shape
    model_width = gain_ref.shape[1]
    hidden_width = gate_hbm.shape[2]
    block_rows = rows // tp_count
    half_cols = down_buf.shape[1]
    half_tp = tp_count // group
    ep_me = lax.axis_index("ep")
    tp_me = lax.axis_index("tp")
    chip_me = ep_me // group
    core_me = ep_me % group
    core_other = 1 - core_me
    partner = (chip_me * group + core_other, tp_me)
    send_table = ((2, 3, 1), (3, 2, 0), (0, 1, 3), (1, 0, 2))
    turn_table = ((0, 3, 2, 1), (1, 3, 2, 0), (2, 0, 1, 3), (3, 0, 1, 2))
    phase_rows = group * cap

    def slot_at(chip, block):
        return pl.ds(pl.multiple_of((chip * tp_count + block) * cap, cap), cap)

    def entry(table, row, column):
        picked = table[0][column]
        for other in range(1, chips):
            picked = jnp.where(row == other, table[other][column], picked)
        return picked

    def turn_at(here, there):
        turn = 0
        for late in range(1, chips):
            turn = jnp.where(entry(turn_table, here, late) == there, late, turn)
        return turn

    def rows_at(turn, core):
        return pl.ds(pl.multiple_of((turn * group + core) * cap, cap), cap)

    def held_at(turn):
        return pl.ds(pl.multiple_of(turn * phase_rows, phase_rows), phase_rows)

    def cols_at(index):
        return pl.ds(pl.multiple_of(index * width, width), width)

    def half_at(core):
        return pl.ds(pl.multiple_of(core * half_cols, half_cols), half_cols)

    def remote(src, dst, send_sem, recv_sem, target):
        return pltpu.make_async_remote_copy(
            src_ref=src,
            dst_ref=dst,
            send_sem=send_sem,
            recv_sem=recv_sem,
            device_id=target,
            device_id_type=pl.DeviceIdType.MESH,
        )

    def settle(ref, sem):
        pltpu.make_async_copy(ref, ref, sem).wait()

    small_loads = [
        pltpu.make_async_copy(ids_hbm, ids_ref, load_sem.at[2]),
        pltpu.make_async_copy(mix_hbm, mix_ref, load_sem.at[3]),
        pltpu.make_async_copy(tok_hbm, tok_ref, load_sem.at[4]),
        pltpu.make_async_copy(gain_hbm, gain_ref, load_sem.at[5]),
    ]
    gate_load = pltpu.make_async_copy(
        gate_hbm.at[0], wide_buf.at[:, pl.ds(0, hidden_width)], load_sem.at[0]
    )
    up_load = pltpu.make_async_copy(
        up_hbm.at[0], wide_buf.at[:, pl.ds(hidden_width, hidden_width)], load_sem.at[1]
    )
    down_load = pltpu.make_async_copy(
        down_hbm.at[0, :, half_at(core_me)],
        down_buf.at[pl.ds(0, hidden_width), :],
        load_sem.at[6],
    )
    for load in small_loads + [gate_load, up_load, down_load]:
        load.start()

    barrier = pltpu.get_barrier_semaphore()
    with jax.named_scope("b_signal"):
        for step_ep in range(ep_count):
            for step_tp in range(tp_count):
                if step_ep or step_tp:
                    pl.semaphore_signal(
                        barrier,
                        inc=1,
                        device_id=(
                            (ep_me + step_ep) % ep_count,
                            (tp_me + step_tp) % tp_count,
                        ),
                        device_id_type=pl.DeviceIdType.MESH,
                    )

    with jax.named_scope("c_pick"):
        row_of = lax.broadcasted_iota(jnp.int32, (rows, rows), 0)
        col_of = lax.broadcasted_iota(jnp.int32, (rows, rows), 1)

        def upright(line):
            return jnp.sum(jnp.where(row_of == col_of, line, 0.0), axis=1, keepdims=True)

        small_loads[0].wait()
        small_loads[1].wait()
        ids = ids_ref[...].astype(jnp.float32)
        mixes = mix_ref[...]
        first_id, second_id = upright(ids[0:1, :]), upright(ids[1:2, :])
        first_mix, second_mix = upright(mixes[0:1, :]), upright(mixes[1:2, :])
        group_of = jnp.zeros((rows, 1), jnp.float32)
        for chip in range(1, chips):
            group_of += (first_id >= chip * group).astype(jnp.float32)
        lanes = lax.broadcasted_iota(jnp.int32, (rows, 128), 1)
        shift = block_rows.bit_length() - 1
        earlier = (col_of < row_of) & ((col_of >> shift) == (row_of >> shift))
        member = (group_of == lanes.astype(jnp.float32)).astype(jnp.float32)
        counts = jnp.dot(
            earlier.astype(jnp.float32).astype(jnp.bfloat16),
            member.astype(jnp.bfloat16),
            preferred_element_type=jnp.float32,
        )
        rank = jnp.sum(counts * member, axis=1, keepdims=True)
        block_of = (lax.broadcasted_iota(jnp.int32, (rows, 1), 0) >> shift).astype(jnp.float32)
        target_slot = (group_of * tp_count + block_of) * cap + rank
        slots = chips * tp_count * cap
        slot_of = lax.broadcasted_iota(jnp.int32, (rows, slots), 1).astype(jnp.float32)
        pick = (slot_of == target_slot).astype(jnp.float32).astype(jnp.bfloat16)
        pick_buf[...] = pick
        across = (((0,), (0,)), ((), ()))
        small_loads[2].wait()
        send_buf[...] = lax.dot_general(
            pick, tok_ref[...], across, preferred_element_type=jnp.float32
        ).astype(jnp.bfloat16)
        in_order = first_id < second_id
        low_mix = jnp.where(in_order, first_mix, second_mix)
        high_mix = jnp.where(in_order, second_mix, first_mix)
        low_top = low_mix.astype(jnp.bfloat16).astype(jnp.float32)
        high_top = high_mix.astype(jnp.bfloat16).astype(jnp.float32)
        mix_cols = jnp.where(lanes == 0, low_top, 0.0)
        mix_cols = jnp.where(lanes == 1, high_top, mix_cols)
        mix_cols = jnp.where(lanes == 2, low_mix - low_top, mix_cols)
        mix_cols = jnp.where(lanes == 3, high_mix - high_top, mix_cols)
        weight_send[...] = lax.dot_general(
            pick, mix_cols.astype(jnp.bfloat16), across, preferred_element_type=jnp.float32
        ).astype(jnp.bfloat16)
        small_loads[3].wait()

    with jax.named_scope("d_barrier"):
        pl.semaphore_wait(barrier, ep_count * tp_count - 1)

    tail_cols = pl.ds(model_width, 128)
    with jax.named_scope("e_issue"):
        for place in (1, 0, 2, 3):
            chip = chip_me if place == 0 else entry(send_table, chip_me, place - 1)
            turn = 0 if place == 0 else turn_at(chip, chip_me)
            src = weight_send.at[slot_at(chip, tp_me)]
            dst = row_buf.at[rows_at(turn, core_me), tail_cols]
            if place == 0:
                pltpu.make_async_copy(src, dst, row_recv_sem.at[turn]).start()
            else:
                remote(
                    src,
                    dst,
                    weight_send_sem.at[0],
                    row_recv_sem.at[turn],
                    (chip * group + core_me, tp_me),
                ).start()
            for step_tp in range(tp_count):
                block = (tp_me + step_tp) % tp_count
                src = send_buf.at[slot_at(chip, block)]
                dst = row_buf.at[rows_at(turn, core_me), cols_at(tp_me)]
                if place == 0 and step_tp == 0:
                    pltpu.make_async_copy(src, dst, row_recv_sem.at[turn]).start()
                else:
                    remote(
                        src,
                        dst,
                        row_send_sem.at[0],
                        row_recv_sem.at[turn],
                        (chip * group + core_me, block),
                    ).start()
        down_copy = remote(
            down_hbm.at[0, :, half_at(core_other)],
            down_buf.at[pl.ds(hidden_width, hidden_width), :],
            down_send_sem.at[0],
            down_recv_sem.at[0],
            partner,
        )
        down_copy.start()

    def receive(turn):
        arrived = row_buf.at[rows_at(turn, core_me)]
        settle(arrived, row_recv_sem.at[turn])
        remote(
            arrived, arrived, pass_send_sem.at[0], pass_recv_sem.at[turn], partner
        ).start()

    def held_by(turns):
        return slice(min(turns) * phase_rows, (max(turns) + 1) * phase_rows)

    def widen(turns):
        held = held_by(turns)
        first = min(turns) == 0
        with jax.named_scope(f"g_passwait{min(turns)}"):
            for turn in turns:
                settle(row_buf.at[rows_at(turn, core_other)], pass_recv_sem.at[turn])
            if first:
                gate_load.wait()
                up_load.wait()
        with jax.named_scope(f"h_gate{min(turns)}"):
            widened = row_buf[held, :model_width].astype(jnp.float32)
            mean_square = jnp.mean(widened * widened, axis=-1, keepdims=True)
            normed = (widened * lax.rsqrt(mean_square + 1e-06) * gain_ref[...]).astype(
                jnp.bfloat16
            )
            both = jnp.dot(normed, wide_buf[...], preferred_element_type=jnp.float32)
            gate_part, up_part = both[:, :hidden_width], both[:, hidden_width:]
            mixes = row_buf[held, model_width:].astype(jnp.float32)
            low = mixes[:, 0:1] + mixes[:, 2:3]
            high = mixes[:, 1:2] + mixes[:, 3:4]
            mix = jnp.where(core_me == 0, low, high)
            hidden = gate_part / (1.0 + jnp.exp(-gate_part)) * up_part * mix
            hidden_buf[held, :hidden_width] = hidden.astype(jnp.bfloat16)
            remote(
                hidden_buf.at[held, :hidden_width],
                hidden_buf.at[held, hidden_width:],
                pair_send_sem.at[0],
                pair_recv_sem.at[min(turns)],
                partner,
            ).start()

    def narrow(turns):
        held = held_by(turns)
        first = min(turns) == 0
        with jax.named_scope(f"l_own{min(turns)}"):
            if first:
                down_load.wait()
            own_part = jnp.dot(
                hidden_buf[held, :hidden_width],
                down_buf[:hidden_width, :],
                preferred_element_type=jnp.float32,
            )
        with jax.named_scope(f"m_hidwait{min(turns)}"):
            settle(hidden_buf.at[held, hidden_width:], pair_recv_sem.at[min(turns)])
            if first:
                down_copy.wait_recv()
        with jax.named_scope(f"n_down{min(turns)}"):
            for part in range(half_tp):
                part_cols = slice(part * width, (part + 1) * width)
                result_buf[held, part_cols] = (
                    own_part[:, part_cols]
                    + jnp.dot(
                        hidden_buf[held, hidden_width:],
                        down_buf[hidden_width:, part_cols],
                        preferred_element_type=jnp.float32,
                    )
                ).astype(jnp.bfloat16)
                feature = core_me * half_tp + part
                for turn in turns:
                    chip = entry(turn_table, chip_me, turn)
                    for step_core in reversed(range(group)):
                        core = (core_me + step_core) % group
                        src = result_buf.at[rows_at(turn, core), part_cols]
                        dst = back_buf.at[slot_at(chip_me, tp_me)]
                        copy = remote(
                            src,
                            dst,
                            back_send_sem.at[0],
                            back_recv_sem.at[0],
                            (chip * group + core, feature),
                        )
                        if step_core == 0 and turn == 0:
                            here = feature == tp_me

                            @pl.when(here)
                            def _():
                                pltpu.make_async_copy(src, dst, back_recv_sem.at[0]).start()

                            @pl.when(jnp.logical_not(here))
                            def _():
                                copy.start()
                        else:
                            copy.start()

    inner = (chip_me + 1) // 2 % 2

    def receive_on(side, turns):
        @pl.when(inner == side)
        def _():
            for turn in turns:
                receive(turn)

    with jax.named_scope("f_recv1"):
        receive(1)
    with jax.named_scope("f_recv0"):
        receive(0)
    widen((1, 0))
    with jax.named_scope("f_recvO"):
        receive_on(0, (2, 3))
    narrow((1, 0))
    with jax.named_scope("f_recvI"):
        receive_on(1, (2, 3))
    widen((2, 3))
    narrow((2, 3))

    with jax.named_scope("o_backwait"):
        settle(back_buf, back_recv_sem.at[0])
    with jax.named_scope("p_out"):
        out_ref[...] = jnp.dot(
            pick_buf[...], back_buf[...], preferred_element_type=jnp.float32
        ).astype(out_ref.dtype)

    with jax.named_scope("q_drain"):
        settle(send_buf.at[pl.ds(0, (chips * tp_count - 1) * cap)], row_send_sem.at[0])
        settle(weight_send.at[pl.ds(0, (chips - 1) * cap)], weight_send_sem.at[0])
        settle(row_buf.at[pl.ds(0, chips * cap)], pass_send_sem.at[0])
        settle(hidden_buf.at[:, :hidden_width], pair_send_sem.at[0])
        down_copy.wait_send()
        stays = tp_me // half_tp == core_me

        @pl.when(stays)
        def _():
            settle(back_buf.at[pl.ds(0, (chips * tp_count - 1) * cap)], back_send_sem.at[0])

        @pl.when(jnp.logical_not(stays))
        def _():
            settle(back_buf, back_send_sem.at[0])


def direct(tokens, norm_gain, gate_weight, up_weight, down_weight, expert_ids, route_weight):
    ep_count, tp_count = lax.axis_size("ep"), lax.axis_size("tp")
    group = math.isqrt(ep_count * gate_weight.shape[0])
    rows, width = tokens.shape
    cap = 4 * (rows // tp_count) // ep_count * group // 2
    chips = ep_count // group
    model_width, hidden_width = gate_weight.shape[1:]
    slots = chips * tp_count * cap
    held = ep_count * cap
    half_cols = model_width // group
    vmem, dma = pltpu.VMEM, pltpu.SemaphoreType.DMA
    low = jnp.bfloat16
    in_vmem = pl.BlockSpec(memory_space=pltpu.VMEM)
    in_hbm = pl.BlockSpec(memory_space=pltpu.HBM)
    return pl.pallas_call(
        partial(direct_kernel, (ep_count, tp_count, group, cap)),
        out_shape=pltpu.VMEM((rows, width), low),
        in_specs=[in_hbm] * 7,
        out_specs=in_vmem,
        scratch_shapes=[
            vmem((2, rows), jnp.int32),
            vmem((2, rows), jnp.float32),
            vmem((rows, width), low),
            vmem((1, model_width), jnp.float32),
            vmem((rows, slots), low),
            vmem((slots, width), low),
            vmem((slots, 128), low),
            vmem((held, model_width + 128), low),
            vmem((model_width, 2 * hidden_width), low),
            vmem((2 * hidden_width, half_cols), low),
            vmem((held, 2 * hidden_width), low),
            vmem((held, half_cols), low),
            vmem((slots, width), low),
            dma((7,)),
            dma((1,)),
            dma((chips,)),
            dma((1,)),
            dma((1,)),
            dma((chips,)),
            dma((1,)),
            dma((chips,)),
            dma((1,)),
            dma((1,)),
            dma((1,)),
            dma((1,)),
        ],
        compiler_params=pltpu.CompilerParams(
            collective_id=0,
            has_side_effects=True,
            vmem_limit_bytes=67043328 - rows * width * 2,
        ),
    )(
        expert_ids.T,
        route_weight.T,
        tokens,
        norm_gain.reshape(1, -1),
        gate_weight,
        up_weight,
        down_weight,
    )


def layer(tokens, norm_gain, gate_weight, up_weight, down_weight, expert_ids, route_weight):
    group = math.isqrt(lax.axis_size("ep") * gate_weight.shape[0])
    paired = group == 2 and gate_weight.shape[0] == 1 and lax.axis_size("ep") == group**3
    body = direct if paired else local
    return body(
        tokens, norm_gain, gate_weight, up_weight, down_weight, expert_ids, route_weight
    )


def solution(mesh):
    in_specs = (
        P("ep", "tp"),
        P(),
        P("ep", None, None),
        P("ep", None, None),
        P("ep", None, None),
        P("ep", None),
        P("ep", None),
    )
    out_specs = P("ep", "tp")
    return jax.shard_map(layer, mesh=mesh, in_specs=in_specs, out_specs=out_specs, check_vma=False)
```

```python
import math
from functools import partial

import jax
import jax.numpy as jnp
from jax import lax
from jax.experimental import pallas as pl
from jax.experimental.pallas import tpu as pltpu
from jax.sharding import PartitionSpec as P


def slot_numbers(block_ids, experts):
    flat_ids = block_ids.reshape(-1)
    hit_table = (flat_ids[:, None] == jnp.arange(experts, dtype=jnp.int32)[None, :]).astype(
        jnp.int32
    )
    earlier = jnp.cumsum(hit_table, axis=0) - hit_table
    return (flat_ids, jnp.sum(earlier * hit_table, axis=1))


def placement_matrix(flat_ids, slot_index, experts, capacity):
    target = (flat_ids * capacity + slot_index).reshape(-1, 2)
    slot_rows = jnp.arange(experts * capacity, dtype=jnp.int32)[:, None]
    first_hit = (target[:, 0][None, :] == slot_rows).astype(jnp.bfloat16)
    second_hit = (target[:, 1][None, :] == slot_rows).astype(jnp.bfloat16)
    return first_hit + second_hit


def expert_apply(row_data, gate_weight, up_weight, down_weight):
    shape_in = row_data.shape
    flat_rows = row_data.reshape(-1, shape_in[-1])
    gate_part = jnp.dot(flat_rows, gate_weight[0], preferred_element_type=jnp.float32)
    up_part = jnp.dot(flat_rows, up_weight[0], preferred_element_type=jnp.float32)
    hidden = (jax.nn.silu(gate_part) * up_part).astype(jnp.bfloat16)
    produced = jnp.dot(hidden, down_weight[0], preferred_element_type=jnp.float32).astype(
        jnp.bfloat16
    )
    return produced.reshape(shape_in[:-1] + (produced.shape[-1],))


def local(tokens, norm_gain, gate_weight, up_weight, down_weight, expert_ids, route_weight):
    tp_count = lax.axis_size("tp")
    experts = lax.axis_size("ep") * gate_weight.shape[0]
    model_width = gate_weight.shape[1]
    group_rows = tokens.shape[0]
    block_rows = group_rows // tp_count
    capacity = 4 * block_rows // experts
    tp_index = lax.axis_index("tp")
    apply_experts = partial(
        expert_apply, gate_weight=gate_weight, up_weight=up_weight, down_weight=down_weight
    )
    full_rows = lax.all_to_all(tokens, "tp", split_axis=0, concat_axis=1, tiled=True)
    block_ids = lax.dynamic_slice_in_dim(expert_ids, tp_index * block_rows, block_rows, 0)
    block_weight = lax.dynamic_slice_in_dim(route_weight, tp_index * block_rows, block_rows, 0)
    widened = full_rows.astype(jnp.float32)
    mean_square = jnp.mean(widened * widened, axis=-1, keepdims=True)
    normed = (widened * lax.rsqrt(mean_square + 1e-06) * norm_gain).astype(jnp.bfloat16)
    flat_ids, slot_index = slot_numbers(block_ids, experts)
    placing = placement_matrix(flat_ids, slot_index, experts, capacity)
    outgoing = jnp.dot(placing, normed, preferred_element_type=jnp.float32).astype(jnp.bfloat16)
    outgoing = outgoing.reshape(experts, capacity, model_width)
    produced = apply_experts(
        lax.all_to_all(outgoing, "ep", split_axis=0, concat_axis=0, tiled=True)
    )
    returned = lax.all_to_all(produced, "ep", split_axis=0, concat_axis=0, tiled=True)
    picked = jnp.take(returned.reshape(-1, model_width), flat_ids * capacity + slot_index, axis=0)
    weighted = picked.astype(jnp.float32) * block_weight.reshape(-1)[:, None]
    mixed_rows = weighted.reshape(block_rows, 2, model_width).sum(axis=1).astype(jnp.bfloat16)
    return lax.all_to_all(mixed_rows, "tp", split_axis=1, concat_axis=0, tiled=True)


def direct_kernel(
    dims,
    ids_hbm,
    mix_hbm,
    tok_hbm,
    gain_hbm,
    gate_hbm,
    up_hbm,
    down_hbm,
    out_ref,
    ids_ref,
    mix_ref,
    tok_ref,
    gain_ref,
    pick_buf,
    send_buf,
    weight_send,
    row_buf,
    wide_buf,
    down_buf,
    hidden_buf,
    result_buf,
    back_buf,
    load_sem,
    row_send_sem,
    row_recv_sem,
    weight_send_sem,
    pass_send_sem,
    pass_recv_sem,
    pair_send_sem,
    pair_recv_sem,
    down_send_sem,
    down_recv_sem,
    back_send_sem,
    back_recv_sem,
):
    ep_count, tp_count, group, cap = dims
    chips = ep_count // group
    rows, width = tok_ref.shape
    model_width = gain_ref.shape[1]
    hidden_width = gate_hbm.shape[2]
    block_rows = rows // tp_count
    half_cols = down_buf.shape[1]
    half_tp = tp_count // group
    ep_me = lax.axis_index("ep")
    tp_me = lax.axis_index("tp")
    chip_me = ep_me // group
    core_me = ep_me % group
    core_other = 1 - core_me
    half_me = core_other
    partner = (chip_me * group + core_other, tp_me)
    send_table = ((3, 2, 1), (3, 2, 0), (0, 1, 3), (1, 0, 2))
    turn_table = ((0, 3, 2, 1), (1, 3, 2, 0), (2, 0, 1, 3), (3, 0, 1, 2))
    phase_rows = group * cap

    def slot_at(chip, block):
        return pl.ds(pl.multiple_of((chip * tp_count + block) * cap, cap), cap)

    def entry(table, row, column):
        picked = table[0][column]
        for other in range(1, chips):
            picked = jnp.where(row == other, table[other][column], picked)
        return picked

    def turn_at(here, there):
        turn = 0
        for late in range(1, chips):
            turn = jnp.where(entry(turn_table, here, late) == there, late, turn)
        return turn

    def rows_at(turn, core):
        return pl.ds(pl.multiple_of((turn * group + core) * cap, cap), cap)

    def held_at(turn):
        return pl.ds(pl.multiple_of(turn * phase_rows, phase_rows), phase_rows)

    def cols_at(index):
        return pl.ds(pl.multiple_of(index * width, width), width)

    def half_at(core):
        return pl.ds(pl.multiple_of(core * half_cols, half_cols), half_cols)

    def remote(src, dst, send_sem, recv_sem, target):
        return pltpu.make_async_remote_copy(
            src_ref=src,
            dst_ref=dst,
            send_sem=send_sem,
            recv_sem=recv_sem,
            device_id=target,
            device_id_type=pl.DeviceIdType.MESH,
        )

    def settle(ref, sem):
        pltpu.make_async_copy(ref, ref, sem).wait()

    small_loads = [
        pltpu.make_async_copy(ids_hbm, ids_ref, load_sem.at[2]),
        pltpu.make_async_copy(mix_hbm, mix_ref, load_sem.at[3]),
        pltpu.make_async_copy(tok_hbm, tok_ref, load_sem.at[4]),
        pltpu.make_async_copy(gain_hbm, gain_ref, load_sem.at[5]),
    ]
    gate_load = pltpu.make_async_copy(
        gate_hbm.at[0], wide_buf.at[:, pl.ds(0, hidden_width)], load_sem.at[0]
    )
    up_load = pltpu.make_async_copy(
        up_hbm.at[0], wide_buf.at[:, pl.ds(hidden_width, hidden_width)], load_sem.at[1]
    )
    down_load = pltpu.make_async_copy(
        down_hbm.at[0, :, half_at(half_me)],
        down_buf.at[pl.ds(0, hidden_width), :],
        load_sem.at[6],
    )
    for load in small_loads + [gate_load, up_load, down_load]:
        load.start()

    barrier = pltpu.get_barrier_semaphore()
    with jax.named_scope("b_signal"):
        for step_ep in range(ep_count):
            for step_tp in range(tp_count):
                if step_ep or step_tp:
                    pl.semaphore_signal(
                        barrier,
                        inc=1,
                        device_id=(
                            (ep_me + step_ep) % ep_count,
                            (tp_me + step_tp) % tp_count,
                        ),
                        device_id_type=pl.DeviceIdType.MESH,
                    )

    with jax.named_scope("c_pick"):
        row_of = lax.broadcasted_iota(jnp.int32, (rows, rows), 0)
        col_of = lax.broadcasted_iota(jnp.int32, (rows, rows), 1)

        def upright(line):
            return jnp.sum(jnp.where(row_of == col_of, line, 0.0), axis=1, keepdims=True)

        small_loads[0].wait()
        small_loads[1].wait()
        ids = ids_ref[...].astype(jnp.float32)
        mixes = mix_ref[...]
        first_id, second_id = upright(ids[0:1, :]), upright(ids[1:2, :])
        first_mix, second_mix = upright(mixes[0:1, :]), upright(mixes[1:2, :])
        group_of = jnp.zeros((rows, 1), jnp.float32)
        for chip in range(1, chips):
            group_of += (first_id >= chip * group).astype(jnp.float32)
        lanes = lax.broadcasted_iota(jnp.int32, (rows, 128), 1)
        shift = block_rows.bit_length() - 1
        earlier = (col_of < row_of) & ((col_of >> shift) == (row_of >> shift))
        member = (group_of == lanes.astype(jnp.float32)).astype(jnp.float32)
        counts = jnp.dot(
            earlier.astype(jnp.float32).astype(jnp.bfloat16),
            member.astype(jnp.bfloat16),
            preferred_element_type=jnp.float32,
        )
        rank = jnp.sum(counts * member, axis=1, keepdims=True)
        block_of = (lax.broadcasted_iota(jnp.int32, (rows, 1), 0) >> shift).astype(jnp.float32)
        target_slot = (group_of * tp_count + block_of) * cap + rank
        slots = chips * tp_count * cap
        slot_of = lax.broadcasted_iota(jnp.int32, (rows, slots), 1).astype(jnp.float32)
        pick = (slot_of == target_slot).astype(jnp.float32).astype(jnp.bfloat16)
        pick_buf[...] = pick
        across = (((0,), (0,)), ((), ()))
        small_loads[2].wait()
        send_buf[...] = lax.dot_general(
            pick, tok_ref[...], across, preferred_element_type=jnp.float32
        ).astype(jnp.bfloat16)
        in_order = first_id < second_id
        low_mix = jnp.where(in_order, first_mix, second_mix)
        high_mix = jnp.where(in_order, second_mix, first_mix)
        low_top = low_mix.astype(jnp.bfloat16).astype(jnp.float32)
        high_top = high_mix.astype(jnp.bfloat16).astype(jnp.float32)
        mix_cols = jnp.where(lanes == 0, low_top, 0.0)
        mix_cols = jnp.where(lanes == 1, high_top, mix_cols)
        mix_cols = jnp.where(lanes == 2, low_mix - low_top, mix_cols)
        mix_cols = jnp.where(lanes == 3, high_mix - high_top, mix_cols)
        weight_send[...] = lax.dot_general(
            pick, mix_cols.astype(jnp.bfloat16), across, preferred_element_type=jnp.float32
        ).astype(jnp.bfloat16)
        small_loads[3].wait()

    with jax.named_scope("d_barrier"):
        pl.semaphore_wait(barrier, ep_count * tp_count - 1)

    tail_cols = pl.ds(model_width, 128)
    with jax.named_scope("e_issue"):
        for place in (1, 0, 2, 3):
            chip = chip_me if place == 0 else entry(send_table, chip_me, place - 1)
            turn = 0 if place == 0 else turn_at(chip, chip_me)
            core = core_me if place == 0 else core_other
            src = weight_send.at[slot_at(chip, tp_me)]
            dst = row_buf.at[rows_at(turn, core), tail_cols]
            if place == 0:
                pltpu.make_async_copy(src, dst, row_recv_sem.at[turn]).start()
            else:
                remote(
                    src,
                    dst,
                    weight_send_sem.at[0],
                    row_recv_sem.at[turn],
                    (chip * group + core, tp_me),
                ).start()
            for step_tp in range(tp_count):
                block = (tp_me + step_tp) % tp_count
                src = send_buf.at[slot_at(chip, block)]
                dst = row_buf.at[rows_at(turn, core), cols_at(tp_me)]
                if place == 0 and step_tp == 0:
                    pltpu.make_async_copy(src, dst, row_recv_sem.at[turn]).start()
                else:
                    remote(
                        src,
                        dst,
                        row_send_sem.at[0],
                        row_recv_sem.at[turn],
                        (chip * group + core, block),
                    ).start()
        down_copy = remote(
            down_hbm.at[0, :, half_at(core_me)],
            down_buf.at[pl.ds(hidden_width, hidden_width), :],
            down_send_sem.at[0],
            down_recv_sem.at[0],
            partner,
        )
        down_copy.start()

    def receive(turn):
        arrived = row_buf.at[rows_at(turn, core_me)]
        settle(arrived, row_recv_sem.at[turn])
        remote(
            arrived, arrived, pass_send_sem.at[0], pass_recv_sem.at[turn], partner
        ).start()

    def held_by(turns):
        return slice(min(turns) * phase_rows, (max(turns) + 1) * phase_rows)

    def widen(turns):
        held = held_by(turns)
        first = min(turns) == 0
        with jax.named_scope(f"g_passwait{min(turns)}"):
            for turn in turns:
                settle(row_buf.at[rows_at(turn, core_other)], pass_recv_sem.at[turn])
            if first:
                gate_load.wait()
                up_load.wait()
        with jax.named_scope(f"h_gate{min(turns)}"):
            widened = row_buf[held, :model_width].astype(jnp.float32)
            mean_square = jnp.mean(widened * widened, axis=-1, keepdims=True)
            normed = (widened * lax.rsqrt(mean_square + 1e-06) * gain_ref[...]).astype(
                jnp.bfloat16
            )
            both = jnp.dot(normed, wide_buf[...], preferred_element_type=jnp.float32)
            gate_part, up_part = both[:, :hidden_width], both[:, hidden_width:]
            mixes = row_buf[held, model_width:].astype(jnp.float32)
            low = mixes[:, 0:1] + mixes[:, 2:3]
            high = mixes[:, 1:2] + mixes[:, 3:4]
            mix = jnp.where(core_me == 0, low, high)
            hidden = gate_part / (1.0 + jnp.exp(-gate_part)) * up_part * mix
            hidden_buf[held, :hidden_width] = hidden.astype(jnp.bfloat16)
            remote(
                hidden_buf.at[held, :hidden_width],
                hidden_buf.at[held, hidden_width:],
                pair_send_sem.at[0],
                pair_recv_sem.at[min(turns)],
                partner,
            ).start()

    def narrow(turns):
        held = held_by(turns)
        first = min(turns) == 0
        with jax.named_scope(f"l_own{min(turns)}"):
            if first:
                down_load.wait()
            own_part = jnp.dot(
                hidden_buf[held, :hidden_width],
                down_buf[:hidden_width, :],
                preferred_element_type=jnp.float32,
            )
        with jax.named_scope(f"m_hidwait{min(turns)}"):
            settle(hidden_buf.at[held, hidden_width:], pair_recv_sem.at[min(turns)])
            if first:
                down_copy.wait_recv()
        with jax.named_scope(f"n_down{min(turns)}"):
            for part in range(half_tp):
                part_cols = slice(part * width, (part + 1) * width)
                result_buf[held, part_cols] = (
                    own_part[:, part_cols]
                    + jnp.dot(
                        hidden_buf[held, hidden_width:],
                        down_buf[hidden_width:, part_cols],
                        preferred_element_type=jnp.float32,
                    )
                ).astype(jnp.bfloat16)
                feature = half_me * half_tp + part
                for turn in turns:
                    chip = entry(turn_table, chip_me, turn)
                    for core in range(group):
                        held_core = core if turn == 0 else 1 - core
                        src = result_buf.at[rows_at(turn, held_core), part_cols]
                        dst = back_buf.at[slot_at(chip_me, tp_me)]
                        copy = remote(
                            src,
                            dst,
                            back_send_sem.at[0],
                            back_recv_sem.at[0],
                            (chip * group + core, feature),
                        )
                        if turn == 0:
                            here = (feature == tp_me) & (core == core_me)

                            @pl.when(here)
                            def _():
                                pltpu.make_async_copy(src, dst, back_recv_sem.at[0]).start()

                            @pl.when(jnp.logical_not(here))
                            def _():
                                copy.start()
                        else:
                            copy.start()

    inner = (chip_me + 1) // 2 % 2

    def receive_on(side, turns):
        @pl.when(inner == side)
        def _():
            for turn in turns:
                receive(turn)

    with jax.named_scope("f_recv1"):
        receive(1)
    with jax.named_scope("f_recv0"):
        receive(0)
    widen((1, 0))
    with jax.named_scope("f_recvO"):
        receive_on(0, (2, 3))
    narrow((1, 0))
    with jax.named_scope("f_recvI"):
        receive_on(1, (2, 3))
    widen((2, 3))
    narrow((2, 3))

    with jax.named_scope("o_backwait"):
        settle(back_buf, back_recv_sem.at[0])
    with jax.named_scope("p_out"):
        out_ref[...] = jnp.dot(
            pick_buf[...], back_buf[...], preferred_element_type=jnp.float32
        ).astype(out_ref.dtype)

    with jax.named_scope("q_drain"):
        settle(send_buf.at[pl.ds(0, (chips * tp_count - 1) * cap)], row_send_sem.at[0])
        settle(weight_send.at[pl.ds(0, (chips - 1) * cap)], weight_send_sem.at[0])
        settle(row_buf.at[pl.ds(0, chips * cap)], pass_send_sem.at[0])
        settle(hidden_buf.at[:, :hidden_width], pair_send_sem.at[0])
        down_copy.wait_send()
        stays = tp_me // half_tp == half_me

        @pl.when(stays)
        def _():
            settle(back_buf.at[pl.ds(0, (chips * tp_count - 1) * cap)], back_send_sem.at[0])

        @pl.when(jnp.logical_not(stays))
        def _():
            settle(back_buf, back_send_sem.at[0])


def direct(tokens, norm_gain, gate_weight, up_weight, down_weight, expert_ids, route_weight):
    ep_count, tp_count = lax.axis_size("ep"), lax.axis_size("tp")
    group = math.isqrt(ep_count * gate_weight.shape[0])
    rows, width = tokens.shape
    cap = 4 * (rows // tp_count) // ep_count * group // 2
    chips = ep_count // group
    model_width, hidden_width = gate_weight.shape[1:]
    slots = chips * tp_count * cap
    held = ep_count * cap
    half_cols = model_width // group
    vmem, dma = pltpu.VMEM, pltpu.SemaphoreType.DMA
    low = jnp.bfloat16
    in_vmem = pl.BlockSpec(memory_space=pltpu.VMEM)
    in_hbm = pl.BlockSpec(memory_space=pltpu.HBM)
    return pl.pallas_call(
        partial(direct_kernel, (ep_count, tp_count, group, cap)),
        out_shape=pltpu.VMEM((rows, width), low),
        in_specs=[in_hbm] * 7,
        out_specs=in_vmem,
        scratch_shapes=[
            vmem((2, rows), jnp.int32),
            vmem((2, rows), jnp.float32),
            vmem((rows, width), low),
            vmem((1, model_width), jnp.float32),
            vmem((rows, slots), low),
            vmem((slots, width), low),
            vmem((slots, 128), low),
            vmem((held, model_width + 128), low),
            vmem((model_width, 2 * hidden_width), low),
            vmem((2 * hidden_width, half_cols), low),
            vmem((held, 2 * hidden_width), low),
            vmem((held, half_cols), low),
            vmem((slots, width), low),
            dma((7,)),
            dma((1,)),
            dma((chips,)),
            dma((1,)),
            dma((1,)),
            dma((chips,)),
            dma((1,)),
            dma((chips,)),
            dma((1,)),
            dma((1,)),
            dma((1,)),
            dma((1,)),
        ],
        compiler_params=pltpu.CompilerParams(
            collective_id=0,
            has_side_effects=True,
            vmem_limit_bytes=67043328 - rows * width * 2,
        ),
    )(
        expert_ids.T,
        route_weight.T,
        tokens,
        norm_gain.reshape(1, -1),
        gate_weight,
        up_weight,
        down_weight,
    )


def layer(tokens, norm_gain, gate_weight, up_weight, down_weight, expert_ids, route_weight):
    group = math.isqrt(lax.axis_size("ep") * gate_weight.shape[0])
    paired = group == 2 and gate_weight.shape[0] == 1 and lax.axis_size("ep") == group**3
    body = direct if paired else local
    return body(
        tokens, norm_gain, gate_weight, up_weight, down_weight, expert_ids, route_weight
    )


def solution(mesh):
    in_specs = (
        P("ep", "tp"),
        P(),
        P("ep", None, None),
        P("ep", None, None),
        P("ep", None, None),
        P("ep", None),
        P("ep", None),
    )
    out_specs = P("ep", "tp")
    return jax.shard_map(layer, mesh=mesh, in_specs=in_specs, out_specs=out_specs, check_vma=False)
```

```python
import math
from functools import partial

import jax
import jax.numpy as jnp
from jax import lax
from jax.experimental import pallas as pl
from jax.experimental.pallas import tpu as pltpu
from jax.sharding import PartitionSpec as P


def slot_numbers(block_ids, experts):
    flat_ids = block_ids.reshape(-1)
    hit_table = (flat_ids[:, None] == jnp.arange(experts, dtype=jnp.int32)[None, :]).astype(
        jnp.int32
    )
    earlier = jnp.cumsum(hit_table, axis=0) - hit_table
    return (flat_ids, jnp.sum(earlier * hit_table, axis=1))


def placement_matrix(flat_ids, slot_index, experts, capacity):
    target = (flat_ids * capacity + slot_index).reshape(-1, 2)
    slot_rows = jnp.arange(experts * capacity, dtype=jnp.int32)[:, None]
    first_hit = (target[:, 0][None, :] == slot_rows).astype(jnp.bfloat16)
    second_hit = (target[:, 1][None, :] == slot_rows).astype(jnp.bfloat16)
    return first_hit + second_hit


def expert_apply(row_data, gate_weight, up_weight, down_weight):
    shape_in = row_data.shape
    flat_rows = row_data.reshape(-1, shape_in[-1])
    gate_part = jnp.dot(flat_rows, gate_weight[0], preferred_element_type=jnp.float32)
    up_part = jnp.dot(flat_rows, up_weight[0], preferred_element_type=jnp.float32)
    hidden = (jax.nn.silu(gate_part) * up_part).astype(jnp.bfloat16)
    produced = jnp.dot(hidden, down_weight[0], preferred_element_type=jnp.float32).astype(
        jnp.bfloat16
    )
    return produced.reshape(shape_in[:-1] + (produced.shape[-1],))


def local(tokens, norm_gain, gate_weight, up_weight, down_weight, expert_ids, route_weight):
    tp_count = lax.axis_size("tp")
    experts = lax.axis_size("ep") * gate_weight.shape[0]
    model_width = gate_weight.shape[1]
    group_rows = tokens.shape[0]
    block_rows = group_rows // tp_count
    capacity = 4 * block_rows // experts
    tp_index = lax.axis_index("tp")
    apply_experts = partial(
        expert_apply, gate_weight=gate_weight, up_weight=up_weight, down_weight=down_weight
    )
    full_rows = lax.all_to_all(tokens, "tp", split_axis=0, concat_axis=1, tiled=True)
    block_ids = lax.dynamic_slice_in_dim(expert_ids, tp_index * block_rows, block_rows, 0)
    block_weight = lax.dynamic_slice_in_dim(route_weight, tp_index * block_rows, block_rows, 0)
    widened = full_rows.astype(jnp.float32)
    mean_square = jnp.mean(widened * widened, axis=-1, keepdims=True)
    normed = (widened * lax.rsqrt(mean_square + 1e-06) * norm_gain).astype(jnp.bfloat16)
    flat_ids, slot_index = slot_numbers(block_ids, experts)
    placing = placement_matrix(flat_ids, slot_index, experts, capacity)
    outgoing = jnp.dot(placing, normed, preferred_element_type=jnp.float32).astype(jnp.bfloat16)
    outgoing = outgoing.reshape(experts, capacity, model_width)
    produced = apply_experts(
        lax.all_to_all(outgoing, "ep", split_axis=0, concat_axis=0, tiled=True)
    )
    returned = lax.all_to_all(produced, "ep", split_axis=0, concat_axis=0, tiled=True)
    picked = jnp.take(returned.reshape(-1, model_width), flat_ids * capacity + slot_index, axis=0)
    weighted = picked.astype(jnp.float32) * block_weight.reshape(-1)[:, None]
    mixed_rows = weighted.reshape(block_rows, 2, model_width).sum(axis=1).astype(jnp.bfloat16)
    return lax.all_to_all(mixed_rows, "tp", split_axis=1, concat_axis=0, tiled=True)


def direct_kernel(
    dims,
    ids_hbm,
    mix_hbm,
    tok_hbm,
    gain_hbm,
    gate_hbm,
    up_hbm,
    down_hbm,
    out_ref,
    ids_ref,
    mix_ref,
    tok_ref,
    gain_ref,
    pick_buf,
    send_buf,
    weight_send,
    row_buf,
    normed_buf,
    wide_buf,
    down_buf,
    hidden_buf,
    result_buf,
    back_buf,
    load_sem,
    row_send_sem,
    row_recv_sem,
    weight_send_sem,
    pass_send_sem,
    pass_recv_sem,
    pair_send_sem,
    pair_recv_sem,
    down_send_sem,
    down_recv_sem,
    back_send_sem,
    back_recv_sem,
):
    ep_count, tp_count, group, cap = dims
    chips = ep_count // group
    rows, width = tok_ref.shape
    model_width = gain_ref.shape[1]
    hidden_width = gate_hbm.shape[2]
    block_rows = rows // tp_count
    half_cols = down_buf.shape[1]
    half_tp = tp_count // group
    ep_me = lax.axis_index("ep")
    tp_me = lax.axis_index("tp")
    chip_me = ep_me // group
    core_me = ep_me % group
    core_other = 1 - core_me
    half_me = core_other
    partner = (chip_me * group + core_other, tp_me)
    send_table = ((3, 2, 1), (3, 2, 0), (0, 1, 3), (1, 0, 2))
    turn_table = ((0, 3, 2, 1), (1, 3, 2, 0), (2, 0, 1, 3), (3, 0, 1, 2))
    phase_rows = group * cap

    def slot_at(chip, block):
        return pl.ds(pl.multiple_of((chip * tp_count + block) * cap, cap), cap)

    def entry(table, row, column):
        picked = table[0][column]
        for other in range(1, chips):
            picked = jnp.where(row == other, table[other][column], picked)
        return picked

    def turn_at(here, there):
        turn = 0
        for late in range(1, chips):
            turn = jnp.where(entry(turn_table, here, late) == there, late, turn)
        return turn

    def across_tp(step):
        block, bit = 0, 1
        while bit < tp_count:
            block, bit = block + (tp_me // bit + step // bit) % 2 * bit, 2 * bit
        return block

    def rows_at(turn, core):
        return pl.ds(pl.multiple_of((turn * group + core) * cap, cap), cap)

    def held_at(turn):
        return pl.ds(pl.multiple_of(turn * phase_rows, phase_rows), phase_rows)

    def cols_at(index):
        return pl.ds(pl.multiple_of(index * width, width), width)

    def half_at(core):
        return pl.ds(pl.multiple_of(core * half_cols, half_cols), half_cols)

    def remote(src, dst, send_sem, recv_sem, target):
        return pltpu.make_async_remote_copy(
            src_ref=src,
            dst_ref=dst,
            send_sem=send_sem,
            recv_sem=recv_sem,
            device_id=target,
            device_id_type=pl.DeviceIdType.MESH,
        )

    def settle(ref, sem):
        pltpu.make_async_copy(ref, ref, sem).wait()

    small_loads = [
        pltpu.make_async_copy(ids_hbm, ids_ref, load_sem.at[2]),
        pltpu.make_async_copy(mix_hbm, mix_ref, load_sem.at[3]),
        pltpu.make_async_copy(tok_hbm, tok_ref, load_sem.at[4]),
        pltpu.make_async_copy(gain_hbm, gain_ref, load_sem.at[5]),
    ]
    gate_load = pltpu.make_async_copy(
        gate_hbm.at[0], wide_buf.at[:, pl.ds(0, hidden_width)], load_sem.at[0]
    )
    up_load = pltpu.make_async_copy(
        up_hbm.at[0], wide_buf.at[:, pl.ds(hidden_width, hidden_width)], load_sem.at[1]
    )
    down_load = pltpu.make_async_copy(
        down_hbm.at[0, :, half_at(half_me)],
        down_buf.at[pl.ds(0, hidden_width), :],
        load_sem.at[6],
    )
    for load in small_loads + [gate_load, up_load, down_load]:
        load.start()

    barrier = pltpu.get_barrier_semaphore()
    with jax.named_scope("b_signal"):
        for step_ep in range(ep_count):
            for step_tp in range(tp_count):
                if step_ep or step_tp:
                    pl.semaphore_signal(
                        barrier,
                        inc=1,
                        device_id=(
                            (ep_me + step_ep) % ep_count,
                            (tp_me + step_tp) % tp_count,
                        ),
                        device_id_type=pl.DeviceIdType.MESH,
                    )

    with jax.named_scope("c_pick"):
        row_of = lax.broadcasted_iota(jnp.int32, (rows, rows), 0)
        col_of = lax.broadcasted_iota(jnp.int32, (rows, rows), 1)

        def upright(line):
            return jnp.sum(jnp.where(row_of == col_of, line, 0.0), axis=1, keepdims=True)

        small_loads[0].wait()
        small_loads[1].wait()
        ids = ids_ref[...].astype(jnp.float32)
        mixes = mix_ref[...]
        first_id, second_id = upright(ids[0:1, :]), upright(ids[1:2, :])
        first_mix, second_mix = upright(mixes[0:1, :]), upright(mixes[1:2, :])
        group_of = jnp.zeros((rows, 1), jnp.float32)
        for chip in range(1, chips):
            group_of += (first_id >= chip * group).astype(jnp.float32)
        lanes = lax.broadcasted_iota(jnp.int32, (rows, 128), 1)
        shift = block_rows.bit_length() - 1
        earlier = (col_of < row_of) & ((col_of >> shift) == (row_of >> shift))
        member = (group_of == lanes.astype(jnp.float32)).astype(jnp.float32)
        counts = jnp.dot(
            earlier.astype(jnp.float32).astype(jnp.bfloat16),
            member.astype(jnp.bfloat16),
            preferred_element_type=jnp.float32,
        )
        rank = jnp.sum(counts * member, axis=1, keepdims=True)
        block_of = (lax.broadcasted_iota(jnp.int32, (rows, 1), 0) >> shift).astype(jnp.float32)
        target_slot = (group_of * tp_count + block_of) * cap + rank
        slots = chips * tp_count * cap
        slot_of = lax.broadcasted_iota(jnp.int32, (rows, slots), 1).astype(jnp.float32)
        pick = (slot_of == target_slot).astype(jnp.float32).astype(jnp.bfloat16)
        pick_buf[...] = pick
        across = (((0,), (0,)), ((), ()))
        small_loads[2].wait()
        send_buf[...] = lax.dot_general(
            pick, tok_ref[...], across, preferred_element_type=jnp.float32
        ).astype(jnp.bfloat16)
        in_order = first_id < second_id
        low_mix = jnp.where(in_order, first_mix, second_mix)
        high_mix = jnp.where(in_order, second_mix, first_mix)
        low_top = low_mix.astype(jnp.bfloat16).astype(jnp.float32)
        high_top = high_mix.astype(jnp.bfloat16).astype(jnp.float32)
        mix_cols = jnp.where(lanes == 0, low_top, 0.0)
        mix_cols = jnp.where(lanes == 1, high_top, mix_cols)
        mix_cols = jnp.where(lanes == 2, low_mix - low_top, mix_cols)
        mix_cols = jnp.where(lanes == 3, high_mix - high_top, mix_cols)
        weight_send[...] = lax.dot_general(
            pick, mix_cols.astype(jnp.bfloat16), across, preferred_element_type=jnp.float32
        ).astype(jnp.bfloat16)
        small_loads[3].wait()

    with jax.named_scope("d_barrier"):
        pl.semaphore_wait(barrier, ep_count * tp_count - 1)

    tail_cols = pl.ds(model_width, 128)
    with jax.named_scope("e_issue"):
        for place in (1, 0, 2, 3):
            chip = chip_me if place == 0 else entry(send_table, chip_me, place - 1)
            turn = 0 if place == 0 else turn_at(chip, chip_me)
            core = core_me if place == 0 else core_other
            for step_tp in (3, 2, 1, 0):
                block = across_tp(step_tp)
                src = send_buf.at[slot_at(chip, block)]
                dst = row_buf.at[rows_at(turn, core), cols_at(tp_me)]
                if place == 0 and step_tp == 0:
                    pltpu.make_async_copy(src, dst, row_recv_sem.at[turn]).start()
                else:
                    remote(
                        src,
                        dst,
                        row_send_sem.at[0],
                        row_recv_sem.at[turn],
                        (chip * group + core, block),
                    ).start()
            src = weight_send.at[slot_at(chip, tp_me)]
            dst = row_buf.at[rows_at(turn, core), tail_cols]
            if place == 0:
                pltpu.make_async_copy(src, dst, row_recv_sem.at[turn]).start()
            else:
                remote(
                    src,
                    dst,
                    weight_send_sem.at[0],
                    row_recv_sem.at[turn],
                    (chip * group + core, tp_me),
                ).start()
        down_copy = remote(
            down_hbm.at[0, :, half_at(core_me)],
            down_buf.at[pl.ds(hidden_width, hidden_width), :],
            down_send_sem.at[0],
            down_recv_sem.at[0],
            partner,
        )
        down_copy.start()

    def receive(turn):
        arrived = row_buf.at[rows_at(turn, core_me)]
        settle(arrived, row_recv_sem.at[turn])
        remote(
            arrived, arrived, pass_send_sem.at[0], pass_recv_sem.at[turn], partner
        ).start()

    def held_by(turns):
        return slice(min(turns) * phase_rows, (max(turns) + 1) * phase_rows)

    def normalize(turns, core):
        for turn in turns:
            picked = rows_at(turn, core)
            widened = row_buf[picked, :model_width].astype(jnp.float32)
            mean_square = jnp.mean(widened * widened, axis=-1, keepdims=True)
            normed_buf[picked, :] = (
                widened * lax.rsqrt(mean_square + 1e-06) * gain_ref[...]
            ).astype(jnp.bfloat16)

    def widen(turns):
        held = held_by(turns)
        first = min(turns) == 0
        with jax.named_scope(f"g_own{min(turns)}"):
            normalize(turns, core_me)
        with jax.named_scope(f"g_passwait{min(turns)}"):
            for turn in turns:
                settle(row_buf.at[rows_at(turn, core_other)], pass_recv_sem.at[turn])
            if first:
                gate_load.wait()
                up_load.wait()
        with jax.named_scope(f"h_gate{min(turns)}"):
            normalize(turns, core_other)
            both = jnp.dot(normed_buf[held, :], wide_buf[...], preferred_element_type=jnp.float32)
            gate_part, up_part = both[:, :hidden_width], both[:, hidden_width:]
            mixes = row_buf[held, model_width:].astype(jnp.float32)
            low = mixes[:, 0:1] + mixes[:, 2:3]
            high = mixes[:, 1:2] + mixes[:, 3:4]
            mix = jnp.where(core_me == 0, low, high)
            hidden = gate_part / (1.0 + jnp.exp(-gate_part)) * up_part * mix
            hidden_buf[held, :hidden_width] = hidden.astype(jnp.bfloat16)
            remote(
                hidden_buf.at[held, :hidden_width],
                hidden_buf.at[held, hidden_width:],
                pair_send_sem.at[0],
                pair_recv_sem.at[min(turns)],
                partner,
            ).start()

    def narrow(turns):
        held = held_by(turns)
        first = min(turns) == 0
        with jax.named_scope(f"l_own{min(turns)}"):
            if first:
                down_load.wait()
            own_part = jnp.dot(
                hidden_buf[held, :hidden_width],
                down_buf[:hidden_width, :],
                preferred_element_type=jnp.float32,
            )
        with jax.named_scope(f"m_hidwait{min(turns)}"):
            settle(hidden_buf.at[held, hidden_width:], pair_recv_sem.at[min(turns)])
            if first:
                down_copy.wait_recv()
        with jax.named_scope(f"n_down{min(turns)}"):
            for part in range(half_tp):
                part_cols = slice(part * width, (part + 1) * width)
                result_buf[held, part_cols] = (
                    own_part[:, part_cols]
                    + jnp.dot(
                        hidden_buf[held, hidden_width:],
                        down_buf[hidden_width:, part_cols],
                        preferred_element_type=jnp.float32,
                    )
                ).astype(jnp.bfloat16)
                feature = half_me * half_tp + part
                for turn in turns:
                    chip = entry(turn_table, chip_me, turn)
                    for core in range(group):
                        held_core = core if turn == 0 else 1 - core
                        src = result_buf.at[rows_at(turn, held_core), part_cols]
                        dst = back_buf.at[slot_at(chip_me, tp_me)]
                        copy = remote(
                            src,
                            dst,
                            back_send_sem.at[0],
                            back_recv_sem.at[0],
                            (chip * group + core, feature),
                        )
                        if turn == 0:
                            here = (feature == tp_me) & (core == core_me)

                            @pl.when(here)
                            def _():
                                pltpu.make_async_copy(src, dst, back_recv_sem.at[0]).start()

                            @pl.when(jnp.logical_not(here))
                            def _():
                                copy.start()
                        else:
                            copy.start()

    inner = (chip_me + 1) // 2 % 2

    def receive_on(side, turns):
        @pl.when(inner == side)
        def _():
            for turn in turns:
                receive(turn)

    with jax.named_scope("f_recv1"):
        receive(1)
    with jax.named_scope("f_recv0"):
        receive(0)
    widen((1, 0))
    with jax.named_scope("f_recvO"):
        receive_on(0, (2, 3))
    narrow((1, 0))
    with jax.named_scope("f_recvI"):
        receive_on(1, (2, 3))
    widen((2, 3))
    narrow((2, 3))

    with jax.named_scope("o_backwait"):
        settle(back_buf, back_recv_sem.at[0])
    with jax.named_scope("p_out"):
        out_ref[...] = jnp.dot(
            pick_buf[...], back_buf[...], preferred_element_type=jnp.float32
        ).astype(out_ref.dtype)

    with jax.named_scope("q_drain"):
        settle(send_buf.at[pl.ds(0, (chips * tp_count - 1) * cap)], row_send_sem.at[0])
        settle(weight_send.at[pl.ds(0, (chips - 1) * cap)], weight_send_sem.at[0])
        settle(row_buf.at[pl.ds(0, chips * cap)], pass_send_sem.at[0])
        settle(hidden_buf.at[:, :hidden_width], pair_send_sem.at[0])
        down_copy.wait_send()
        stays = tp_me // half_tp == half_me

        @pl.when(stays)
        def _():
            settle(back_buf.at[pl.ds(0, (chips * tp_count - 1) * cap)], back_send_sem.at[0])

        @pl.when(jnp.logical_not(stays))
        def _():
            settle(back_buf, back_send_sem.at[0])


def direct(tokens, norm_gain, gate_weight, up_weight, down_weight, expert_ids, route_weight):
    ep_count, tp_count = lax.axis_size("ep"), lax.axis_size("tp")
    group = math.isqrt(ep_count * gate_weight.shape[0])
    rows, width = tokens.shape
    cap = 4 * (rows // tp_count) // ep_count * group // 2
    chips = ep_count // group
    model_width, hidden_width = gate_weight.shape[1:]
    slots = chips * tp_count * cap
    held = ep_count * cap
    half_cols = model_width // group
    vmem, dma = pltpu.VMEM, pltpu.SemaphoreType.DMA
    low = jnp.bfloat16
    in_vmem = pl.BlockSpec(memory_space=pltpu.VMEM)
    in_hbm = pl.BlockSpec(memory_space=pltpu.HBM)
    return pl.pallas_call(
        partial(direct_kernel, (ep_count, tp_count, group, cap)),
        out_shape=pltpu.VMEM((rows, width), low),
        in_specs=[in_hbm] * 7,
        out_specs=in_vmem,
        scratch_shapes=[
            vmem((2, rows), jnp.int32),
            vmem((2, rows), jnp.float32),
            vmem((rows, width), low),
            vmem((1, model_width), jnp.float32),
            vmem((rows, slots), low),
            vmem((slots, width), low),
            vmem((slots, 128), low),
            vmem((held, model_width + 128), low),
            vmem((held, model_width), low),
            vmem((model_width, 2 * hidden_width), low),
            vmem((2 * hidden_width, half_cols), low),
            vmem((held, 2 * hidden_width), low),
            vmem((held, half_cols), low),
            vmem((slots, width), low),
            dma((7,)),
            dma((1,)),
            dma((chips,)),
            dma((1,)),
            dma((1,)),
            dma((chips,)),
            dma((1,)),
            dma((chips,)),
            dma((1,)),
            dma((1,)),
            dma((1,)),
            dma((1,)),
        ],
        compiler_params=pltpu.CompilerParams(
            collective_id=0,
            has_side_effects=True,
            vmem_limit_bytes=67043328 - rows * width * 2,
        ),
    )(
        expert_ids.T,
        route_weight.T,
        tokens,
        norm_gain.reshape(1, -1),
        gate_weight,
        up_weight,
        down_weight,
    )


def layer(tokens, norm_gain, gate_weight, up_weight, down_weight, expert_ids, route_weight):
    group = math.isqrt(lax.axis_size("ep") * gate_weight.shape[0])
    paired = group == 2 and gate_weight.shape[0] == 1 and lax.axis_size("ep") == group**3
    body = direct if paired else local
    return body(
        tokens, norm_gain, gate_weight, up_weight, down_weight, expert_ids, route_weight
    )


def solution(mesh):
    in_specs = (
        P("ep", "tp"),
        P(),
        P("ep", None, None),
        P("ep", None, None),
        P("ep", None, None),
        P("ep", None),
        P("ep", None),
    )
    out_specs = P("ep", "tp")
    return jax.shard_map(layer, mesh=mesh, in_specs=in_specs, out_specs=out_specs, check_vma=False)
```

```python
import math
from functools import partial

import jax
import jax.numpy as jnp
from jax import lax
from jax.experimental import pallas as pl
from jax.experimental.pallas import tpu as pltpu
from jax.sharding import PartitionSpec as P


def slot_numbers(block_ids, experts):
    flat_ids = block_ids.reshape(-1)
    hit_table = (flat_ids[:, None] == jnp.arange(experts, dtype=jnp.int32)[None, :]).astype(
        jnp.int32
    )
    earlier = jnp.cumsum(hit_table, axis=0) - hit_table
    return (flat_ids, jnp.sum(earlier * hit_table, axis=1))


def placement_matrix(flat_ids, slot_index, experts, capacity):
    target = (flat_ids * capacity + slot_index).reshape(-1, 2)
    slot_rows = jnp.arange(experts * capacity, dtype=jnp.int32)[:, None]
    first_hit = (target[:, 0][None, :] == slot_rows).astype(jnp.bfloat16)
    second_hit = (target[:, 1][None, :] == slot_rows).astype(jnp.bfloat16)
    return first_hit + second_hit


def expert_apply(row_data, gate_weight, up_weight, down_weight):
    shape_in = row_data.shape
    flat_rows = row_data.reshape(-1, shape_in[-1])
    gate_part = jnp.dot(flat_rows, gate_weight[0], preferred_element_type=jnp.float32)
    up_part = jnp.dot(flat_rows, up_weight[0], preferred_element_type=jnp.float32)
    hidden = (jax.nn.silu(gate_part) * up_part).astype(jnp.bfloat16)
    produced = jnp.dot(hidden, down_weight[0], preferred_element_type=jnp.float32).astype(
        jnp.bfloat16
    )
    return produced.reshape(shape_in[:-1] + (produced.shape[-1],))


def local(tokens, norm_gain, gate_weight, up_weight, down_weight, expert_ids, route_weight):
    tp_count = lax.axis_size("tp")
    experts = lax.axis_size("ep") * gate_weight.shape[0]
    model_width = gate_weight.shape[1]
    group_rows = tokens.shape[0]
    block_rows = group_rows // tp_count
    capacity = 4 * block_rows // experts
    tp_index = lax.axis_index("tp")
    apply_experts = partial(
        expert_apply, gate_weight=gate_weight, up_weight=up_weight, down_weight=down_weight
    )
    full_rows = lax.all_to_all(tokens, "tp", split_axis=0, concat_axis=1, tiled=True)
    block_ids = lax.dynamic_slice_in_dim(expert_ids, tp_index * block_rows, block_rows, 0)
    block_weight = lax.dynamic_slice_in_dim(route_weight, tp_index * block_rows, block_rows, 0)
    widened = full_rows.astype(jnp.float32)
    mean_square = jnp.mean(widened * widened, axis=-1, keepdims=True)
    normed = (widened * lax.rsqrt(mean_square + 1e-06) * norm_gain).astype(jnp.bfloat16)
    flat_ids, slot_index = slot_numbers(block_ids, experts)
    placing = placement_matrix(flat_ids, slot_index, experts, capacity)
    outgoing = jnp.dot(placing, normed, preferred_element_type=jnp.float32).astype(jnp.bfloat16)
    outgoing = outgoing.reshape(experts, capacity, model_width)
    produced = apply_experts(
        lax.all_to_all(outgoing, "ep", split_axis=0, concat_axis=0, tiled=True)
    )
    returned = lax.all_to_all(produced, "ep", split_axis=0, concat_axis=0, tiled=True)
    picked = jnp.take(returned.reshape(-1, model_width), flat_ids * capacity + slot_index, axis=0)
    weighted = picked.astype(jnp.float32) * block_weight.reshape(-1)[:, None]
    mixed_rows = weighted.reshape(block_rows, 2, model_width).sum(axis=1).astype(jnp.bfloat16)
    return lax.all_to_all(mixed_rows, "tp", split_axis=1, concat_axis=0, tiled=True)


def direct_kernel(
    dims,
    ids_hbm,
    mix_hbm,
    tok_hbm,
    gain_hbm,
    gate_hbm,
    up_hbm,
    down_hbm,
    out_ref,
    ids_ref,
    mix_ref,
    tok_ref,
    gain_ref,
    pick_buf,
    send_buf,
    weight_send,
    row_buf,
    normed_buf,
    wide_buf,
    down_buf,
    hidden_buf,
    result_buf,
    back_buf,
    load_sem,
    row_send_sem,
    row_recv_sem,
    weight_send_sem,
    pass_send_sem,
    pass_recv_sem,
    pair_send_sem,
    pair_recv_sem,
    down_send_sem,
    down_recv_sem,
    back_send_sem,
    back_recv_sem,
):
    ep_count, tp_count, group, cap = dims
    chips = ep_count // group
    rows, width = tok_ref.shape
    model_width = gain_ref.shape[1]
    hidden_width = gate_hbm.shape[2]
    block_rows = rows // tp_count
    half_cols = down_buf.shape[1]
    half_tp = tp_count // group
    ep_me = lax.axis_index("ep")
    tp_me = lax.axis_index("tp")
    chip_me = ep_me // group
    core_me = ep_me % group
    core_other = 1 - core_me
    half_me = core_other
    partner = (chip_me * group + core_other, tp_me)
    send_table = ((3, 2, 1), (3, 2, 0), (0, 1, 3), (1, 0, 2))
    turn_table = ((0, 3, 2, 1), (1, 3, 0, 2), (2, 0, 1, 3), (3, 0, 1, 2))
    phase_rows = group * cap

    def slot_at(chip, block):
        return pl.ds(pl.multiple_of((chip * tp_count + block) * cap, cap), cap)

    def entry(table, row, column):
        picked = table[0][column]
        for other in range(1, chips):
            picked = jnp.where(row == other, table[other][column], picked)
        return picked

    def turn_at(here, there):
        turn = 0
        for late in range(1, chips):
            turn = jnp.where(entry(turn_table, here, late) == there, late, turn)
        return turn

    def across_tp(step):
        block, bit = 0, 1
        while bit < tp_count:
            block, bit = block + (tp_me // bit + step // bit) % 2 * bit, 2 * bit
        return block

    def rows_at(turn, core):
        return pl.ds(pl.multiple_of((turn * group + core) * cap, cap), cap)

    def held_at(turn):
        return pl.ds(pl.multiple_of(turn * phase_rows, phase_rows), phase_rows)

    def cols_at(index):
        return pl.ds(pl.multiple_of(index * width, width), width)

    def half_at(core):
        return pl.ds(pl.multiple_of(core * half_cols, half_cols), half_cols)

    def remote(src, dst, send_sem, recv_sem, target):
        return pltpu.make_async_remote_copy(
            src_ref=src,
            dst_ref=dst,
            send_sem=send_sem,
            recv_sem=recv_sem,
            device_id=target,
            device_id_type=pl.DeviceIdType.MESH,
        )

    def settle(ref, sem):
        pltpu.make_async_copy(ref, ref, sem).wait()

    small_loads = [
        pltpu.make_async_copy(ids_hbm, ids_ref, load_sem.at[2]),
        pltpu.make_async_copy(mix_hbm, mix_ref, load_sem.at[3]),
        pltpu.make_async_copy(tok_hbm, tok_ref, load_sem.at[4]),
        pltpu.make_async_copy(gain_hbm, gain_ref, load_sem.at[5]),
    ]
    gate_load = pltpu.make_async_copy(
        gate_hbm.at[0], wide_buf.at[:, pl.ds(0, hidden_width)], load_sem.at[0]
    )
    up_load = pltpu.make_async_copy(
        up_hbm.at[0], wide_buf.at[:, pl.ds(hidden_width, hidden_width)], load_sem.at[1]
    )
    down_load = pltpu.make_async_copy(
        down_hbm.at[0, :, half_at(half_me)],
        down_buf.at[pl.ds(0, hidden_width), :],
        load_sem.at[6],
    )
    for load in small_loads + [gate_load, up_load, down_load]:
        load.start()

    barrier = pltpu.get_barrier_semaphore()
    with jax.named_scope("b_signal"):
        for step_ep in range(ep_count):
            for step_tp in range(tp_count):
                if step_ep or step_tp:
                    pl.semaphore_signal(
                        barrier,
                        inc=1,
                        device_id=(
                            (ep_me + step_ep) % ep_count,
                            (tp_me + step_tp) % tp_count,
                        ),
                        device_id_type=pl.DeviceIdType.MESH,
                    )

    with jax.named_scope("c_pick"):
        row_of = lax.broadcasted_iota(jnp.int32, (rows, rows), 0)
        col_of = lax.broadcasted_iota(jnp.int32, (rows, rows), 1)

        def upright(line):
            return jnp.sum(jnp.where(row_of == col_of, line, 0.0), axis=1, keepdims=True)

        small_loads[0].wait()
        small_loads[1].wait()
        ids = ids_ref[...].astype(jnp.float32)
        mixes = mix_ref[...]
        first_id, second_id = upright(ids[0:1, :]), upright(ids[1:2, :])
        first_mix, second_mix = upright(mixes[0:1, :]), upright(mixes[1:2, :])
        group_of = jnp.zeros((rows, 1), jnp.float32)
        for chip in range(1, chips):
            group_of += (first_id >= chip * group).astype(jnp.float32)
        lanes = lax.broadcasted_iota(jnp.int32, (rows, 128), 1)
        shift = block_rows.bit_length() - 1
        earlier = (col_of < row_of) & ((col_of >> shift) == (row_of >> shift))
        member = (group_of == lanes.astype(jnp.float32)).astype(jnp.float32)
        counts = jnp.dot(
            earlier.astype(jnp.float32).astype(jnp.bfloat16),
            member.astype(jnp.bfloat16),
            preferred_element_type=jnp.float32,
        )
        rank = jnp.sum(counts * member, axis=1, keepdims=True)
        block_of = (lax.broadcasted_iota(jnp.int32, (rows, 1), 0) >> shift).astype(jnp.float32)
        target_slot = (group_of * tp_count + block_of) * cap + rank
        slots = chips * tp_count * cap
        slot_of = lax.broadcasted_iota(jnp.int32, (rows, slots), 1).astype(jnp.float32)
        pick = (slot_of == target_slot).astype(jnp.float32).astype(jnp.bfloat16)
        pick_buf[...] = pick
        across = (((0,), (0,)), ((), ()))
        small_loads[2].wait()
        send_buf[...] = lax.dot_general(
            pick, tok_ref[...], across, preferred_element_type=jnp.float32
        ).astype(jnp.bfloat16)
        in_order = first_id < second_id
        low_mix = jnp.where(in_order, first_mix, second_mix)
        high_mix = jnp.where(in_order, second_mix, first_mix)
        low_top = low_mix.astype(jnp.bfloat16).astype(jnp.float32)
        high_top = high_mix.astype(jnp.bfloat16).astype(jnp.float32)
        mix_cols = jnp.where(lanes == 0, low_top, 0.0)
        mix_cols = jnp.where(lanes == 1, high_top, mix_cols)
        mix_cols = jnp.where(lanes == 2, low_mix - low_top, mix_cols)
        mix_cols = jnp.where(lanes == 3, high_mix - high_top, mix_cols)
        weight_send[...] = lax.dot_general(
            pick, mix_cols.astype(jnp.bfloat16), across, preferred_element_type=jnp.float32
        ).astype(jnp.bfloat16)
        small_loads[3].wait()

    with jax.named_scope("d_barrier"):
        pl.semaphore_wait(barrier, ep_count * tp_count - 1)

    tail_cols = pl.ds(model_width, 128)
    with jax.named_scope("e_issue"):
        for place in (1, 0, 2, 3):
            chip = chip_me if place == 0 else entry(send_table, chip_me, place - 1)
            turn = 0 if place == 0 else turn_at(chip, chip_me)
            core = core_me if place == 0 else core_other
            for step_tp in (3, 2, 1, 0):
                block = across_tp(step_tp)
                src = send_buf.at[slot_at(chip, block)]
                dst = row_buf.at[rows_at(turn, core), cols_at(tp_me)]
                if place == 0 and step_tp == 0:
                    pltpu.make_async_copy(src, dst, row_recv_sem.at[turn]).start()
                else:
                    remote(
                        src,
                        dst,
                        row_send_sem.at[0],
                        row_recv_sem.at[turn],
                        (chip * group + core, block),
                    ).start()
            src = weight_send.at[slot_at(chip, tp_me)]
            dst = row_buf.at[rows_at(turn, core), tail_cols]
            if place == 0:
                pltpu.make_async_copy(src, dst, row_recv_sem.at[turn]).start()
            else:
                remote(
                    src,
                    dst,
                    weight_send_sem.at[0],
                    row_recv_sem.at[turn],
                    (chip * group + core, tp_me),
                ).start()
        down_copy = remote(
            down_hbm.at[0, :, half_at(core_me)],
            down_buf.at[pl.ds(hidden_width, hidden_width), :],
            down_send_sem.at[0],
            down_recv_sem.at[0],
            partner,
        )
        down_copy.start()

    def receive(turn):
        arrived = row_buf.at[rows_at(turn, core_me)]
        settle(arrived, row_recv_sem.at[turn])
        remote(
            arrived, arrived, pass_send_sem.at[0], pass_recv_sem.at[turn], partner
        ).start()

    def held_by(turns):
        return slice(min(turns) * phase_rows, (max(turns) + 1) * phase_rows)

    def normalize(turns, core):
        for turn in turns:
            picked = rows_at(turn, core)
            widened = row_buf[picked, :model_width].astype(jnp.float32)
            mean_square = jnp.mean(widened * widened, axis=-1, keepdims=True)
            normed_buf[picked, :] = (
                widened * lax.rsqrt(mean_square + 1e-06) * gain_ref[...]
            ).astype(jnp.bfloat16)

    def widen(turns):
        held = held_by(turns)
        first = min(turns) == 0
        with jax.named_scope(f"g_own{min(turns)}"):
            normalize(turns, core_me)
        with jax.named_scope(f"g_passwait{min(turns)}"):
            for turn in turns:
                settle(row_buf.at[rows_at(turn, core_other)], pass_recv_sem.at[turn])
            if first:
                gate_load.wait()
                up_load.wait()
        with jax.named_scope(f"h_gate{min(turns)}"):
            normalize(turns, core_other)
            both = jnp.dot(normed_buf[held, :], wide_buf[...], preferred_element_type=jnp.float32)
            gate_part, up_part = both[:, :hidden_width], both[:, hidden_width:]
            mixes = row_buf[held, model_width:].astype(jnp.float32)
            low = mixes[:, 0:1] + mixes[:, 2:3]
            high = mixes[:, 1:2] + mixes[:, 3:4]
            mix = jnp.where(core_me == 0, low, high)
            hidden = gate_part / (1.0 + jnp.exp(-gate_part)) * up_part * mix
            hidden_buf[held, :hidden_width] = hidden.astype(jnp.bfloat16)
            remote(
                hidden_buf.at[held, :hidden_width],
                hidden_buf.at[held, hidden_width:],
                pair_send_sem.at[0],
                pair_recv_sem.at[min(turns)],
                partner,
            ).start()

    def narrow(turns):
        held = held_by(turns)
        first = min(turns) == 0
        with jax.named_scope(f"l_own{min(turns)}"):
            if first:
                down_load.wait()
            own_part = jnp.dot(
                hidden_buf[held, :hidden_width],
                down_buf[:hidden_width, :],
                preferred_element_type=jnp.float32,
            )
        with jax.named_scope(f"m_hidwait{min(turns)}"):
            settle(hidden_buf.at[held, hidden_width:], pair_recv_sem.at[min(turns)])
            if first:
                down_copy.wait_recv()
        with jax.named_scope(f"n_down{min(turns)}"):
            for part in range(half_tp):
                part_cols = slice(part * width, (part + 1) * width)
                result_buf[held, part_cols] = (
                    own_part[:, part_cols]
                    + jnp.dot(
                        hidden_buf[held, hidden_width:],
                        down_buf[hidden_width:, part_cols],
                        preferred_element_type=jnp.float32,
                    )
                ).astype(jnp.bfloat16)
                feature = half_me * half_tp + part
                for turn in turns:
                    chip = entry(turn_table, chip_me, turn)
                    for core in range(group):
                        held_core = core if turn == 0 else 1 - core
                        src = result_buf.at[rows_at(turn, held_core), part_cols]
                        dst = back_buf.at[slot_at(chip_me, tp_me)]
                        copy = remote(
                            src,
                            dst,
                            back_send_sem.at[0],
                            back_recv_sem.at[0],
                            (chip * group + core, feature),
                        )
                        if turn == 0:
                            here = (feature == tp_me) & (core == core_me)

                            @pl.when(here)
                            def _():
                                pltpu.make_async_copy(src, dst, back_recv_sem.at[0]).start()

                            @pl.when(jnp.logical_not(here))
                            def _():
                                copy.start()
                        else:
                            copy.start()

    inner = (chip_me + 1) // 2 % 2

    def receive_on(side, turns):
        @pl.when(inner == side)
        def _():
            for turn in turns:
                receive(turn)

    with jax.named_scope("f_recv0"):
        receive(0)
    with jax.named_scope("f_recv1"):
        receive(1)
    widen((1, 0))
    with jax.named_scope("f_recvO"):
        receive_on(0, (2, 3))
    narrow((1, 0))
    with jax.named_scope("f_recvI"):
        receive_on(1, (2, 3))
    widen((2, 3))
    narrow((2, 3))

    with jax.named_scope("o_backwait"):
        settle(back_buf, back_recv_sem.at[0])
    with jax.named_scope("p_out"):
        out_ref[...] = jnp.dot(
            pick_buf[...], back_buf[...], preferred_element_type=jnp.float32
        ).astype(out_ref.dtype)

    with jax.named_scope("q_drain"):
        settle(send_buf.at[pl.ds(0, (chips * tp_count - 1) * cap)], row_send_sem.at[0])
        settle(weight_send.at[pl.ds(0, (chips - 1) * cap)], weight_send_sem.at[0])
        settle(row_buf.at[pl.ds(0, chips * cap)], pass_send_sem.at[0])
        settle(hidden_buf.at[:, :hidden_width], pair_send_sem.at[0])
        down_copy.wait_send()
        stays = tp_me // half_tp == half_me

        @pl.when(stays)
        def _():
            settle(back_buf.at[pl.ds(0, (chips * tp_count - 1) * cap)], back_send_sem.at[0])

        @pl.when(jnp.logical_not(stays))
        def _():
            settle(back_buf, back_send_sem.at[0])


def direct(tokens, norm_gain, gate_weight, up_weight, down_weight, expert_ids, route_weight):
    ep_count, tp_count = lax.axis_size("ep"), lax.axis_size("tp")
    group = math.isqrt(ep_count * gate_weight.shape[0])
    rows, width = tokens.shape
    cap = 4 * (rows // tp_count) // ep_count * group // 2
    chips = ep_count // group
    model_width, hidden_width = gate_weight.shape[1:]
    slots = chips * tp_count * cap
    held = ep_count * cap
    half_cols = model_width // group
    vmem, dma = pltpu.VMEM, pltpu.SemaphoreType.DMA
    low = jnp.bfloat16
    in_vmem = pl.BlockSpec(memory_space=pltpu.VMEM)
    in_hbm = pl.BlockSpec(memory_space=pltpu.HBM)
    return pl.pallas_call(
        partial(direct_kernel, (ep_count, tp_count, group, cap)),
        out_shape=pltpu.VMEM((rows, width), low),
        in_specs=[in_hbm] * 7,
        out_specs=in_vmem,
        scratch_shapes=[
            vmem((2, rows), jnp.int32),
            vmem((2, rows), jnp.float32),
            vmem((rows, width), low),
            vmem((1, model_width), jnp.float32),
            vmem((rows, slots), low),
            vmem((slots, width), low),
            vmem((slots, 128), low),
            vmem((held, model_width + 128), low),
            vmem((held, model_width), low),
            vmem((model_width, 2 * hidden_width), low),
            vmem((2 * hidden_width, half_cols), low),
            vmem((held, 2 * hidden_width), low),
            vmem((held, half_cols), low),
            vmem((slots, width), low),
            dma((7,)),
            dma((1,)),
            dma((chips,)),
            dma((1,)),
            dma((1,)),
            dma((chips,)),
            dma((1,)),
            dma((chips,)),
            dma((1,)),
            dma((1,)),
            dma((1,)),
            dma((1,)),
        ],
        compiler_params=pltpu.CompilerParams(
            collective_id=0,
            has_side_effects=True,
            vmem_limit_bytes=67043328 - rows * width * 2,
        ),
    )(
        expert_ids.T,
        route_weight.T,
        tokens,
        norm_gain.reshape(1, -1),
        gate_weight,
        up_weight,
        down_weight,
    )


def layer(tokens, norm_gain, gate_weight, up_weight, down_weight, expert_ids, route_weight):
    group = math.isqrt(lax.axis_size("ep") * gate_weight.shape[0])
    paired = group == 2 and gate_weight.shape[0] == 1 and lax.axis_size("ep") == group**3
    body = direct if paired else local
    return body(
        tokens, norm_gain, gate_weight, up_weight, down_weight, expert_ids, route_weight
    )


def solution(mesh):
    in_specs = (
        P("ep", "tp"),
        P(),
        P("ep", None, None),
        P("ep", None, None),
        P("ep", None, None),
        P("ep", None),
        P("ep", None),
    )
    out_specs = P("ep", "tp")
    return jax.shard_map(layer, mesh=mesh, in_specs=in_specs, out_specs=out_specs, check_vma=False)
```

```python
import math
from functools import partial

import jax
import jax.numpy as jnp
from jax import lax
from jax.experimental import pallas as pl
from jax.experimental.pallas import tpu as pltpu
from jax.sharding import PartitionSpec as P


def slot_numbers(block_ids, experts):
    flat_ids = block_ids.reshape(-1)
    hit_table = (flat_ids[:, None] == jnp.arange(experts, dtype=jnp.int32)[None, :]).astype(
        jnp.int32
    )
    earlier = jnp.cumsum(hit_table, axis=0) - hit_table
    return (flat_ids, jnp.sum(earlier * hit_table, axis=1))


def placement_matrix(flat_ids, slot_index, experts, capacity):
    target = (flat_ids * capacity + slot_index).reshape(-1, 2)
    slot_rows = jnp.arange(experts * capacity, dtype=jnp.int32)[:, None]
    first_hit = (target[:, 0][None, :] == slot_rows).astype(jnp.bfloat16)
    second_hit = (target[:, 1][None, :] == slot_rows).astype(jnp.bfloat16)
    return first_hit + second_hit


def expert_apply(row_data, gate_weight, up_weight, down_weight):
    shape_in = row_data.shape
    flat_rows = row_data.reshape(-1, shape_in[-1])
    gate_part = jnp.dot(flat_rows, gate_weight[0], preferred_element_type=jnp.float32)
    up_part = jnp.dot(flat_rows, up_weight[0], preferred_element_type=jnp.float32)
    hidden = (jax.nn.silu(gate_part) * up_part).astype(jnp.bfloat16)
    produced = jnp.dot(hidden, down_weight[0], preferred_element_type=jnp.float32).astype(
        jnp.bfloat16
    )
    return produced.reshape(shape_in[:-1] + (produced.shape[-1],))


def local(tokens, norm_gain, gate_weight, up_weight, down_weight, expert_ids, route_weight):
    tp_count = lax.axis_size("tp")
    experts = lax.axis_size("ep") * gate_weight.shape[0]
    model_width = gate_weight.shape[1]
    group_rows = tokens.shape[0]
    block_rows = group_rows // tp_count
    capacity = 4 * block_rows // experts
    tp_index = lax.axis_index("tp")
    apply_experts = partial(
        expert_apply, gate_weight=gate_weight, up_weight=up_weight, down_weight=down_weight
    )
    full_rows = lax.all_to_all(tokens, "tp", split_axis=0, concat_axis=1, tiled=True)
    block_ids = lax.dynamic_slice_in_dim(expert_ids, tp_index * block_rows, block_rows, 0)
    block_weight = lax.dynamic_slice_in_dim(route_weight, tp_index * block_rows, block_rows, 0)
    widened = full_rows.astype(jnp.float32)
    mean_square = jnp.mean(widened * widened, axis=-1, keepdims=True)
    normed = (widened * lax.rsqrt(mean_square + 1e-06) * norm_gain).astype(jnp.bfloat16)
    flat_ids, slot_index = slot_numbers(block_ids, experts)
    placing = placement_matrix(flat_ids, slot_index, experts, capacity)
    outgoing = jnp.dot(placing, normed, preferred_element_type=jnp.float32).astype(jnp.bfloat16)
    outgoing = outgoing.reshape(experts, capacity, model_width)
    produced = apply_experts(
        lax.all_to_all(outgoing, "ep", split_axis=0, concat_axis=0, tiled=True)
    )
    returned = lax.all_to_all(produced, "ep", split_axis=0, concat_axis=0, tiled=True)
    picked = jnp.take(returned.reshape(-1, model_width), flat_ids * capacity + slot_index, axis=0)
    weighted = picked.astype(jnp.float32) * block_weight.reshape(-1)[:, None]
    mixed_rows = weighted.reshape(block_rows, 2, model_width).sum(axis=1).astype(jnp.bfloat16)
    return lax.all_to_all(mixed_rows, "tp", split_axis=1, concat_axis=0, tiled=True)


def direct_kernel(
    dims,
    ids_hbm,
    mix_hbm,
    tok_hbm,
    gain_hbm,
    gate_hbm,
    up_hbm,
    down_hbm,
    out_ref,
    ids_ref,
    mix_ref,
    tok_ref,
    gain_ref,
    pick_buf,
    send_buf,
    weight_send,
    row_buf,
    normed_buf,
    wide_buf,
    down_buf,
    hidden_buf,
    result_buf,
    back_buf,
    load_sem,
    row_send_sem,
    row_recv_sem,
    weight_send_sem,
    pass_send_sem,
    pass_recv_sem,
    pair_send_sem,
    pair_recv_sem,
    down_send_sem,
    down_recv_sem,
    back_send_sem,
    back_recv_sem,
):
    ep_count, tp_count, group, cap = dims
    chips = ep_count // group
    rows, width = tok_ref.shape
    model_width = gain_ref.shape[1]
    hidden_width = gate_hbm.shape[2]
    block_rows = rows // tp_count
    half_cols = down_buf.shape[1]
    half_tp = tp_count // group
    ep_me = lax.axis_index("ep")
    tp_me = lax.axis_index("tp")
    chip_me = ep_me // group
    core_me = ep_me % group
    core_other = 1 - core_me
    half_me = core_other
    partner = (chip_me * group + core_other, tp_me)
    send_table = ((3, 2, 1), (3, 2, 0), (0, 1, 3), (1, 0, 2))
    turn_table = ((0, 3, 2, 1), (1, 3, 0, 2), (2, 0, 1, 3), (3, 0, 1, 2))
    phase_rows = group * cap

    def slot_at(chip, block):
        return pl.ds(pl.multiple_of((chip * tp_count + block) * cap, cap), cap)

    def entry(table, row, column):
        picked = table[0][column]
        for other in range(1, chips):
            picked = jnp.where(row == other, table[other][column], picked)
        return picked

    def turn_at(here, there):
        turn = 0
        for late in range(1, chips):
            turn = jnp.where(entry(turn_table, here, late) == there, late, turn)
        return turn

    def across_tp(step):
        block, bit = 0, 1
        while bit < tp_count:
            block, bit = block + (tp_me // bit + step // bit) % 2 * bit, 2 * bit
        return block

    def rows_at(turn, core):
        return pl.ds(pl.multiple_of((turn * group + core) * cap, cap), cap)

    def held_at(turn):
        return pl.ds(pl.multiple_of(turn * phase_rows, phase_rows), phase_rows)

    def cols_at(index):
        return pl.ds(pl.multiple_of(index * width, width), width)

    def half_at(core):
        return pl.ds(pl.multiple_of(core * half_cols, half_cols), half_cols)

    def remote(src, dst, send_sem, recv_sem, target):
        return pltpu.make_async_remote_copy(
            src_ref=src,
            dst_ref=dst,
            send_sem=send_sem,
            recv_sem=recv_sem,
            device_id=target,
            device_id_type=pl.DeviceIdType.MESH,
        )

    def settle(ref, sem):
        pltpu.make_async_copy(ref, ref, sem).wait()

    small_loads = [
        pltpu.make_async_copy(ids_hbm, ids_ref, load_sem.at[2]),
        pltpu.make_async_copy(mix_hbm, mix_ref, load_sem.at[3]),
        pltpu.make_async_copy(tok_hbm, tok_ref, load_sem.at[4]),
        pltpu.make_async_copy(gain_hbm, gain_ref, load_sem.at[5]),
    ]
    gate_load = pltpu.make_async_copy(
        gate_hbm.at[0], wide_buf.at[:, pl.ds(0, hidden_width)], load_sem.at[0]
    )
    up_load = pltpu.make_async_copy(
        up_hbm.at[0], wide_buf.at[:, pl.ds(hidden_width, hidden_width)], load_sem.at[0]
    )
    down_load = pltpu.make_async_copy(
        down_hbm.at[0, :, half_at(half_me)],
        down_buf.at[pl.ds(0, hidden_width), :],
        load_sem.at[1],
    )
    for load in small_loads + [gate_load, up_load, down_load]:
        load.start()

    barrier = pltpu.get_barrier_semaphore()
    with jax.named_scope("b_signal"):
        for step_ep in (*range(1, ep_count), 0):
            for step_tp in range(tp_count):
                if step_ep or step_tp:
                    pl.semaphore_signal(
                        barrier,
                        inc=1,
                        device_id=(
                            (ep_me + step_ep) % ep_count,
                            (tp_me + step_tp) % tp_count,
                        ),
                        device_id_type=pl.DeviceIdType.MESH,
                    )

    with jax.named_scope("c_pick"):
        row_of = lax.broadcasted_iota(jnp.int32, (rows, rows), 0)
        col_of = lax.broadcasted_iota(jnp.int32, (rows, rows), 1)

        def upright(line):
            return jnp.sum(jnp.where(row_of == col_of, line, 0.0), axis=1, keepdims=True)

        small_loads[0].wait()
        small_loads[1].wait()
        ids = ids_ref[...].astype(jnp.float32)
        mixes = mix_ref[...]
        first_id, second_id = upright(ids[0:1, :]), upright(ids[1:2, :])
        first_mix, second_mix = upright(mixes[0:1, :]), upright(mixes[1:2, :])
        group_of = jnp.zeros((rows, 1), jnp.float32)
        for chip in range(1, chips):
            group_of += (first_id >= chip * group).astype(jnp.float32)
        lanes = lax.broadcasted_iota(jnp.int32, (rows, 128), 1)
        shift = block_rows.bit_length() - 1
        earlier = (col_of < row_of) & ((col_of >> shift) == (row_of >> shift))
        member = (group_of == lanes.astype(jnp.float32)).astype(jnp.float32)
        counts = jnp.dot(
            earlier.astype(jnp.float32).astype(jnp.bfloat16),
            member.astype(jnp.bfloat16),
            preferred_element_type=jnp.float32,
        )
        rank = jnp.sum(counts * member, axis=1, keepdims=True)
        block_of = (lax.broadcasted_iota(jnp.int32, (rows, 1), 0) >> shift).astype(jnp.float32)
        target_slot = (group_of * tp_count + block_of) * cap + rank
        slots = chips * tp_count * cap
        slot_of = lax.broadcasted_iota(jnp.int32, (rows, slots), 1).astype(jnp.float32)
        pick = (slot_of == target_slot).astype(jnp.float32).astype(jnp.bfloat16)
        pick_buf[...] = pick
        across = (((0,), (0,)), ((), ()))
        small_loads[2].wait()
        send_buf[...] = lax.dot_general(
            pick, tok_ref[...], across, preferred_element_type=jnp.float32
        ).astype(jnp.bfloat16)
        in_order = first_id < second_id
        low_mix = jnp.where(in_order, first_mix, second_mix)
        high_mix = jnp.where(in_order, second_mix, first_mix)
        low_top = low_mix.astype(jnp.bfloat16).astype(jnp.float32)
        high_top = high_mix.astype(jnp.bfloat16).astype(jnp.float32)
        mix_cols = jnp.where(lanes == 0, low_top, 0.0)
        mix_cols = jnp.where(lanes == 1, high_top, mix_cols)
        mix_cols = jnp.where(lanes == 2, low_mix - low_top, mix_cols)
        mix_cols = jnp.where(lanes == 3, high_mix - high_top, mix_cols)
        weight_send[...] = lax.dot_general(
            pick, mix_cols.astype(jnp.bfloat16), across, preferred_element_type=jnp.float32
        ).astype(jnp.bfloat16)
        small_loads[3].wait()

    with jax.named_scope("d_barrier"):
        pl.semaphore_wait(barrier, ep_count * tp_count - 1)

    tail_cols = pl.ds(model_width, 128)
    with jax.named_scope("e_issue"):
        for place in (1, 0, 2, 3):
            chip = chip_me if place == 0 else entry(send_table, chip_me, place - 1)
            turn = 0 if place == 0 else turn_at(chip, chip_me)
            core = core_me if place == 0 else core_other
            for step_tp in (3, 2, 1, 0):
                block = across_tp(step_tp)
                src = send_buf.at[slot_at(chip, block)]
                dst = row_buf.at[rows_at(turn, core), cols_at(tp_me)]
                if place == 0 and step_tp == 0:
                    pltpu.make_async_copy(src, dst, row_recv_sem.at[turn]).start()
                else:
                    remote(
                        src,
                        dst,
                        row_send_sem.at[0],
                        row_recv_sem.at[turn],
                        (chip * group + core, block),
                    ).start()
            src = weight_send.at[slot_at(chip, tp_me)]
            dst = row_buf.at[rows_at(turn, core), tail_cols]
            if place == 0:
                pltpu.make_async_copy(src, dst, row_recv_sem.at[turn]).start()
            else:
                remote(
                    src,
                    dst,
                    weight_send_sem.at[0],
                    row_recv_sem.at[turn],
                    (chip * group + core, tp_me),
                ).start()
        down_copy = remote(
            down_hbm.at[0, :, half_at(core_me)],
            down_buf.at[pl.ds(hidden_width, hidden_width), :],
            down_send_sem.at[0],
            down_recv_sem.at[0],
            partner,
        )
        down_copy.start()

    def receive(turn):
        arrived = row_buf.at[rows_at(turn, core_me)]
        settle(arrived, row_recv_sem.at[turn])
        remote(
            arrived, arrived, pass_send_sem.at[0], pass_recv_sem.at[turn], partner
        ).start()

    def held_by(turns):
        return slice(min(turns) * phase_rows, (max(turns) + 1) * phase_rows)

    def normalize(turns, core):
        for turn in turns:
            picked = rows_at(turn, core)
            widened = row_buf[picked, :model_width].astype(jnp.float32)
            mean_square = jnp.mean(widened * widened, axis=-1, keepdims=True)
            normed_buf[picked, :] = (
                widened * lax.rsqrt(mean_square + 1e-06) * gain_ref[...]
            ).astype(jnp.bfloat16)

    def widen(turns):
        held = held_by(turns)
        first = min(turns) == 0
        with jax.named_scope(f"g_own{min(turns)}"):
            normalize(turns, core_me)
        with jax.named_scope(f"g_passwait{min(turns)}"):
            for turn in turns:
                settle(row_buf.at[rows_at(turn, core_other)], pass_recv_sem.at[turn])
            if first:
                settle(wide_buf, load_sem.at[0])
        with jax.named_scope(f"h_gate{min(turns)}"):
            normalize(turns, core_other)
            both = jnp.dot(normed_buf[held, :], wide_buf[...], preferred_element_type=jnp.float32)
            gate_part, up_part = both[:, :hidden_width], both[:, hidden_width:]
            mixes = row_buf[held, model_width:].astype(jnp.float32)
            low = mixes[:, 0:1] + mixes[:, 2:3]
            high = mixes[:, 1:2] + mixes[:, 3:4]
            mix = jnp.where(core_me == 0, low, high)
            hidden = gate_part / (1.0 + jnp.exp(-gate_part)) * up_part * mix
            hidden_buf[held, :hidden_width] = hidden.astype(jnp.bfloat16)
            remote(
                hidden_buf.at[held, :hidden_width],
                hidden_buf.at[held, hidden_width:],
                pair_send_sem.at[0],
                pair_recv_sem.at[min(turns)],
                partner,
            ).start()

    def narrow(turns):
        held = held_by(turns)
        first = min(turns) == 0
        with jax.named_scope(f"l_own{min(turns)}"):
            if first:
                down_load.wait()
            own_part = jnp.dot(
                hidden_buf[held, :hidden_width],
                down_buf[:hidden_width, :],
                preferred_element_type=jnp.float32,
            )
        with jax.named_scope(f"m_hidwait{min(turns)}"):
            settle(hidden_buf.at[held, hidden_width:], pair_recv_sem.at[min(turns)])
            if first:
                down_copy.wait_recv()
        with jax.named_scope(f"n_down{min(turns)}"):
            for part in range(half_tp):
                part_cols = slice(part * width, (part + 1) * width)
                result_buf[held, part_cols] = (
                    own_part[:, part_cols]
                    + jnp.dot(
                        hidden_buf[held, hidden_width:],
                        down_buf[hidden_width:, part_cols],
                        preferred_element_type=jnp.float32,
                    )
                ).astype(jnp.bfloat16)
                feature = half_me * half_tp + part
                for turn in turns:
                    chip = entry(turn_table, chip_me, turn)
                    for core in range(group):
                        held_core = core if turn == 0 else 1 - core
                        src = result_buf.at[rows_at(turn, held_core), part_cols]
                        dst = back_buf.at[slot_at(chip_me, tp_me)]
                        copy = remote(
                            src,
                            dst,
                            back_send_sem.at[0],
                            back_recv_sem.at[0],
                            (chip * group + core, feature),
                        )
                        if turn == 0:
                            here = (feature == tp_me) & (core == core_me)

                            @pl.when(here)
                            def _():
                                pltpu.make_async_copy(src, dst, back_recv_sem.at[0]).start()

                            @pl.when(jnp.logical_not(here))
                            def _():
                                copy.start()
                        else:
                            copy.start()

    inner = (chip_me + 1) // 2 % 2

    def receive_on(side, turns):
        @pl.when(inner == side)
        def _():
            for turn in turns:
                receive(turn)

    with jax.named_scope("f_recv0"):
        receive(0)
    with jax.named_scope("f_recv1"):
        receive(1)
    widen((1, 0))
    with jax.named_scope("f_recvO"):
        receive_on(0, (2, 3))
    narrow((1, 0))
    with jax.named_scope("f_recvI"):
        receive_on(1, (2, 3))
    widen((2, 3))
    narrow((2, 3))

    with jax.named_scope("o_backwait"):
        settle(back_buf, back_recv_sem.at[0])
    with jax.named_scope("p_out"):
        out_ref[...] = jnp.dot(
            pick_buf[...], back_buf[...], preferred_element_type=jnp.float32
        ).astype(out_ref.dtype)

    with jax.named_scope("q_drain"):
        settle(send_buf.at[pl.ds(0, (chips * tp_count - 1) * cap)], row_send_sem.at[0])
        settle(weight_send.at[pl.ds(0, (chips - 1) * cap)], weight_send_sem.at[0])
        settle(row_buf.at[pl.ds(0, chips * cap)], pass_send_sem.at[0])
        settle(hidden_buf.at[:, :hidden_width], pair_send_sem.at[0])
        down_copy.wait_send()
        stays = tp_me // half_tp == half_me

        @pl.when(stays)
        def _():
            settle(back_buf.at[pl.ds(0, (chips * tp_count - 1) * cap)], back_send_sem.at[0])

        @pl.when(jnp.logical_not(stays))
        def _():
            settle(back_buf, back_send_sem.at[0])


def direct(tokens, norm_gain, gate_weight, up_weight, down_weight, expert_ids, route_weight):
    ep_count, tp_count = lax.axis_size("ep"), lax.axis_size("tp")
    group = math.isqrt(ep_count * gate_weight.shape[0])
    rows, width = tokens.shape
    cap = 4 * (rows // tp_count) // ep_count * group // 2
    chips = ep_count // group
    model_width, hidden_width = gate_weight.shape[1:]
    slots = chips * tp_count * cap
    held = ep_count * cap
    half_cols = model_width // group
    vmem, dma = pltpu.VMEM, pltpu.SemaphoreType.DMA
    low = jnp.bfloat16
    in_vmem = pl.BlockSpec(memory_space=pltpu.VMEM)
    in_hbm = pl.BlockSpec(memory_space=pltpu.HBM)
    return pl.pallas_call(
        partial(direct_kernel, (ep_count, tp_count, group, cap)),
        out_shape=pltpu.VMEM((rows, width), low),
        in_specs=[in_hbm] * 7,
        out_specs=in_vmem,
        scratch_shapes=[
            vmem((2, rows), jnp.int32),
            vmem((2, rows), jnp.float32),
            vmem((rows, width), low),
            vmem((1, model_width), jnp.float32),
            vmem((rows, slots), low),
            vmem((slots, width), low),
            vmem((slots, 128), low),
            vmem((held, model_width + 128), low),
            vmem((held, model_width), low),
            vmem((model_width, 2 * hidden_width), low),
            vmem((2 * hidden_width, half_cols), low),
            vmem((held, 2 * hidden_width), low),
            vmem((held, half_cols), low),
            vmem((slots, width), low),
            dma((6,)),
            dma((1,)),
            dma((chips,)),
            dma((1,)),
            dma((1,)),
            dma((chips,)),
            dma((1,)),
            dma((chips,)),
            dma((1,)),
            dma((1,)),
            dma((1,)),
            dma((1,)),
        ],
        compiler_params=pltpu.CompilerParams(
            collective_id=0,
            has_side_effects=True,
            vmem_limit_bytes=67043328 - rows * width * 2,
        ),
    )(
        expert_ids.T,
        route_weight.T,
        tokens,
        norm_gain.reshape(1, -1),
        gate_weight,
        up_weight,
        down_weight,
    )


def layer(tokens, norm_gain, gate_weight, up_weight, down_weight, expert_ids, route_weight):
    group = math.isqrt(lax.axis_size("ep") * gate_weight.shape[0])
    paired = group == 2 and gate_weight.shape[0] == 1 and lax.axis_size("ep") == group**3
    body = direct if paired else local
    return body(
        tokens, norm_gain, gate_weight, up_weight, down_weight, expert_ids, route_weight
    )


def solution(mesh):
    in_specs = (
        P("ep", "tp"),
        P(),
        P("ep", None, None),
        P("ep", None, None),
        P("ep", None, None),
        P("ep", None),
        P("ep", None),
    )
    out_specs = P("ep", "tp")
    return jax.shard_map(layer, mesh=mesh, in_specs=in_specs, out_specs=out_specs, check_vma=False)
```
